32 devices in a mesh: sp: 16 (over z, y, core), tp: 2 (over x).
Axes of the slice: x: 2, y: 2, z: 4, core: 2. Of those that a mesh axis runs over, the one named last changes fastest.
Arguments:
- target: bfloat16 [2048, 2048], P('sp'), may hold values from -0.375 to 0.375
- source: bfloat16 [4096, 2048], P(('sp', 'tp')), may hold values from -0.375 to 0.375
- target_gain: float32 [2048], replicated, may hold values from 0.3 to 12
- source_gain: float32 [2048], replicated, may hold values from 0.3 to 12
- w_query: bfloat16 [2048, 1024], P(None, 'tp'), may hold values from -0.125 to 0.125
- w_key: bfloat16 [2048, 256], replicated, may hold values from -0.125 to 0.125
- w_value: bfloat16 [2048, 256], replicated, may hold values from -0.125 to 0.125
- attended: bfloat16 [2048, 1024], P('sp', 'tp'), may hold values from -6 to 6
- d_attended: bfloat16 [2048, 1024], P('sp', 'tp'), may hold values from -24 to 24
Outputs:
- d_target: bfloat16 [2048, 2048], P('sp')
- d_source: float32 [4096, 2048], P(('sp', 'tp'))
- d_w_query: float32 [2048, 1024], P('sp', 'tp')
The draws below stay inside these ranges and needn't reach their ends.
All inputs are finite; a program needn't handle non-finite values.
Results may differ from the reference program's by a relative error of at most 0.02.
The reference program's roundings to bfloat16 on the way count: a program that leaves them out, or rounds other values in their place, can miss the bound.
Values may be sent and summed in bfloat16 or wider, within the bound.
No kernel may reach another device: no remote copies, remote signals or barrier semaphores. Data moves between devices by JAX's collectives and lax.ppermute only.
A program may use at most 64 MiB of HBM per device.

```python
import jax
import jax.numpy as jnp
from jax import lax

D = 2048
HQ = 8
KVH = 2
HD = 128
TT = 2048
SS = 4096


def gain_law(key):
    return jax.random.uniform(key, (D,), jnp.float32, 0.3, 1.7)


def draw_target_gain(key, part):
    return gain_law(jax.random.fold_in(key, 11))


def draw_source_gain(key, part):
    return gain_law(jax.random.fold_in(key, 23))


def level_of(rng, extent, pieces, least, largest):
    factor_of = 1.0
    for position, parts in pieces:
        heights = jax.random.uniform(jax.random.fold_in(jax.random.fold_in(rng, 6), position), (parts,), jnp.float32, least / len(pieces), largest / len(pieces))
        factor_of = factor_of * jnp.repeat(jnp.exp(heights), extent[position] // parts).reshape((-1,) + (1,) * (len(extent) - 1 - position))
    return factor_of


def gaussian(key, dims, deviation, most, shards=(), held_as=jnp.bfloat16):
    loudness = level_of(key, dims, shards, -0.22, 0.18) if shards else 1.0
    array = jax.random.normal(key, dims, jnp.float32) * deviation * loudness
    return jnp.minimum(jnp.maximum(array, -most), most).astype(held_as)


def setup_inputs(seed: int = 0) -> dict:
    key_of = jax.random.split(jax.random.key(seed), 10)
    target = gaussian(key_of[0], (TT, D), 0.0625, 0.375, ((0, 16),))
    source = gaussian(key_of[1], (SS, D), 0.0625, 0.375, ((0, 32),))
    target_gain = draw_target_gain(jax.random.fold_in(key_of[9], 71), 0)
    source_gain = draw_source_gain(jax.random.fold_in(key_of[9], 71), 0)
    w_query = gaussian(key_of[4], (D, HQ * HD), D ** -0.5, 0.125, ((1, 2),))
    w_key = gaussian(key_of[5], (D, KVH * HD), D ** -0.5, 0.125)
    w_value = gaussian(key_of[6], (D, KVH * HD), D ** -0.5, 0.125)
    attended = gaussian(key_of[7], (TT, HQ * HD), 1.0, 6.0, ((0, 16), (1, 2)))
    d_attended = gaussian(key_of[8], (TT, HQ * HD), 4.0, 24.0, ((0, 16), (1, 2)))
    return {"target": target, "source": source, "target_gain": target_gain, "source_gain": source_gain, "w_query": w_query, "w_key": w_key, "w_value": w_value, "attended": attended, "d_attended": d_attended}


EPS = 1e-06

def norm_rows(matrix, gain_vector):
    widened = matrix.astype(jnp.float32)
    inverse = lax.rsqrt(lax.optimization_barrier(jnp.mean(widened * widened, axis=-1, keepdims=True)) + EPS)
    return widened * inverse * gain_vector

def norm_back(matrix, gain_vector, cotangent):
    _, pullback = jax.vjp(lambda values: norm_rows(values, gain_vector), matrix.astype(jnp.float32))
    return pullback(cotangent)[0]

def block_count(row_count, most_rows):
    number = 1
    while row_count % (number * 2) == 0 and row_count // number > most_rows:
        number = number * 2
    return number

def reference(target, source, target_gain, source_gain, w_query, w_key, w_value, attended, d_attended):
    scaling = HD ** (-0.5)
    group_size = HQ // KVH
    normed_target = norm_rows(target, target_gain).astype(jnp.bfloat16)
    normed_source = norm_rows(source, source_gain).astype(jnp.bfloat16)
    query = jnp.dot(normed_target, w_query, preferred_element_type=jnp.float32).astype(jnp.bfloat16)
    key = jnp.dot(normed_source, w_key, preferred_element_type=jnp.float32).astype(jnp.bfloat16)
    value = jnp.dot(normed_source, w_value, preferred_element_type=jnp.float32).astype(jnp.bfloat16)
    target_total = query.shape[0]
    source_total = key.shape[0]
    delta = lax.optimization_barrier(jnp.sum(d_attended.astype(jnp.float32).reshape(target_total, HQ, HD) * attended.astype(jnp.float32).reshape(target_total, HQ, HD), axis=-1)).astype(jnp.bfloat16)
    number = block_count(target_total, 512)
    block_rows = target_total // number

    def one_head(head_index):
        kv_index = head_index // group_size
        query_head = lax.dynamic_slice_in_dim(query, head_index * HD, HD, 1)
        key_head = lax.dynamic_slice_in_dim(key, kv_index * HD, HD, 1)
        value_head = lax.dynamic_slice_in_dim(value, kv_index * HD, HD, 1)
        grad_head = lax.dynamic_slice_in_dim(d_attended, head_index * HD, HD, 1)
        delta_head = lax.dynamic_slice_in_dim(delta, head_index, 1, 1)[:, 0]
        query_blocks = query_head.reshape(number, block_rows, HD)
        grad_blocks = grad_head.reshape(number, block_rows, HD)
        delta_blocks = delta_head.reshape(number, block_rows)

        def totals_of(queries):
            scores = jnp.dot(queries, key_head.T, preferred_element_type=jnp.float32) * scaling
            maxima = lax.optimization_barrier(jnp.max(scores, axis=-1))
            return maxima + jnp.log(lax.optimization_barrier(jnp.sum(jnp.exp(scores - maxima[:, None]), axis=-1)))
        log_total = lax.map(totals_of, query_blocks)

        def grad_step(carried, blocks):
            queries, cotangent, totals, delta_rows = blocks
            scores = jnp.dot(queries, key_head.T, preferred_element_type=jnp.float32) * scaling
            weights = jnp.exp(scores - totals[:, None])
            d_weights = jnp.dot(cotangent, value_head.T, preferred_element_type=jnp.float32)
            d_scores = (weights * (d_weights - delta_rows.astype(jnp.float32)[:, None])).astype(jnp.bfloat16)
            query_grad = jnp.dot(d_scores, key_head, preferred_element_type=jnp.float32) * scaling
            key_acc = carried[0] + jnp.dot(d_scores.T, queries, preferred_element_type=jnp.float32) * scaling
            value_acc = carried[1] + jnp.dot(weights.astype(jnp.bfloat16).T, cotangent, preferred_element_type=jnp.float32)
            return ((key_acc, value_acc), query_grad)
        start_state = (jnp.zeros((source_total, HD), jnp.float32), jnp.zeros((source_total, HD), jnp.float32))
        (key_acc, value_acc), query_grads = lax.scan(grad_step, start_state, (query_blocks, grad_blocks, log_total, delta_blocks))
        return (key_acc, value_acc, query_grads.reshape(target_total, HD))
    key_grads, value_grads, query_grads = lax.map(one_head, jnp.arange(HQ, dtype=jnp.int32))
    d_key = key_grads.reshape(KVH, group_size, source_total, HD).sum(axis=1)
    d_value = value_grads.reshape(KVH, group_size, source_total, HD).sum(axis=1)
    d_key_b = d_key.transpose(1, 0, 2).reshape(source_total, KVH * HD).astype(jnp.bfloat16)
    d_value_b = d_value.transpose(1, 0, 2).reshape(source_total, KVH * HD).astype(jnp.bfloat16)
    d_query_b = query_grads.transpose(1, 0, 2).reshape(target_total, HQ * HD).astype(jnp.bfloat16)
    d_w_query = jnp.dot(normed_target.T, d_query_b, preferred_element_type=jnp.float32)
    d_normed_target = jnp.dot(d_query_b, w_query.T, preferred_element_type=jnp.float32)
    d_target = norm_back(target, target_gain, d_normed_target).astype(jnp.bfloat16)
    d_normed_source = jnp.dot(d_key_b, w_key.T, preferred_element_type=jnp.float32) + jnp.dot(d_value_b, w_value.T, preferred_element_type=jnp.float32)
    d_source = norm_back(source, source_gain, d_normed_source)
    return (d_target, d_source, d_w_query)
```

```python
import functools

import jax
import jax.numpy as jnp
from jax import lax
from jax.experimental import pallas as pl
from jax.experimental.pallas import tpu as pltpu
from jax.sharding import PartitionSpec as P

KVH = 2
HD = 128
EPS = 1e-06
LOG2E = 1.4426950408889634


F32 = jnp.float32
BF16 = jnp.bfloat16


def swap(x, axis, k):
    n = lax.axis_size(axis)
    return lax.ppermute(x, axis, [(i, i ^ k) for i in range(n)])


def norm_parts(matrix):
    widened = matrix.astype(F32)
    inverse = lax.rsqrt(jnp.mean(widened * widened, axis=-1, keepdims=True) + EPS)
    return widened, inverse


def norm_rows(matrix, gain_vector):
    widened, inverse = norm_parts(matrix)
    return (widened * inverse * gain_vector).astype(BF16)


def norm_back(matrix, gain_vector, cotangent):
    widened, inverse = norm_parts(matrix)
    scaled = cotangent * gain_vector
    inner = jnp.mean(widened * scaled, axis=-1, keepdims=True)
    return inverse * scaled - widened * (inverse * inverse * inverse * inner)


def dot(a, b, ca, cb):
    return lax.dot_general(a, b, (((ca,), (cb,)), ((), ())), preferred_element_type=F32)


def params(mb=60):
    return pltpu.CompilerParams(
        vmem_limit_bytes=mb * 1024 * 1024, dimension_semantics=("arbitrary",)
    )


def scores_kernel(nz, nb, rows, scaling, *refs):
    kvs, qs, (p_ref, st_ref) = refs[:nz], refs[nz : nz + nb], refs[nz + nb :]
    src = kvs[0].shape[0]
    for pair in range(nb // 2):
        q = jnp.concatenate([qs[2 * pair][:rows, :], qs[2 * pair + 1][:rows, :]], axis=0)
        cols = slice(pair * 2 * rows, (pair + 1) * 2 * rows)
        parts = [dot(kv[:, :HD], q, 1, 1) for kv in kvs]
        top = functools.reduce(
            jnp.maximum, [jnp.max(s, axis=0, keepdims=True) for s in parts]
        )
        total = jnp.zeros_like(top)
        for z, s in enumerate(parts):
            p = jnp.exp2((s - top) * (scaling * LOG2E))
            total = total + jnp.sum(p, axis=0, keepdims=True)
            p_ref[0, z * src : (z + 1) * src, cols] = p.astype(BF16)
        st_ref[0, 0:1, cols] = top * (scaling * LOG2E)
        st_ref[0, 1:2, cols] = total


def grads_kernel(nz, nb, rows, *refs):
    kvs, qs, gs = refs[:nz], refs[nz : nz + nb], refs[nz + nb : nz + 2 * nb]
    p_ref, ds_ref, dq_ref = refs[nz + 2 * nb :]
    src = kvs[0].shape[0]
    for pair in range(nb // 2):
        a, b = 2 * pair, 2 * pair + 1
        g = jnp.concatenate([gs[a][...], gs[b][...]], axis=0)
        delta = jnp.concatenate(
            [qs[a][rows : rows + 1, :], qs[b][rows : rows + 1, :]], axis=1
        ).astype(F32)
        cols = slice(pair * 2 * rows, (pair + 1) * 2 * rows)
        acc = None
        for z, kv in enumerate(kvs):
            dw = dot(kv[:, HD:], g, 1, 1)
            p = p_ref[0, z * src : (z + 1) * src, cols].astype(F32)
            ds = (p * (dw - delta)).astype(BF16)
            ds_ref[0, z * src : (z + 1) * src, cols] = ds
            part = dot(kv[:, :HD], ds, 0, 0)
            acc = part if acc is None else acc + part
        dq_ref[0, :, cols] = acc


def scale_kernel(nb, rows, heads, scaling, *refs):
    sts = refs[:nb]
    dq_ref, c_ref = refs[nb], refs[nb + 1]
    outs = refs[nb + 2 :]
    for h in range(heads):
        own_top = sts[0][h, 0:1, :]
        tops, sums = [own_top], [sts[0][h, 1:2, :]]
        for k in range(1, nb):
            order = [j ^ k for j in range(nb)]
            tops.append(
                jnp.concatenate([sts[k][h, 0:1, o * rows : (o + 1) * rows] for o in order], axis=1)
            )
            sums.append(
                jnp.concatenate([sts[k][h, 1:2, o * rows : (o + 1) * rows] for o in order], axis=1)
            )
        top = functools.reduce(jnp.maximum, tops)
        total = sum(s * jnp.exp2(t - top) for t, s in zip(tops, sums))
        c = jnp.exp2(own_top - top) / total
        c_ref[h, 0:1, :] = c
        for k in range(nb):
            part = slice(k * rows, (k + 1) * rows)
            block = dq_ref[h, :, part] * (c[:, part] * scaling)
            outs[k][:, h * HD : (h + 1) * HD] = block.T.astype(BF16)


def keyvalue_kernel(nz, nb, rows, scaling, *refs):
    qs, gs = refs[:nb], refs[nb : 2 * nb]
    c_ref, p_ref, ds_ref = refs[2 * nb : 2 * nb + 3]
    outs = refs[2 * nb + 3 : 2 * nb + 3 + nz]
    acc = refs[2 * nb + 3 + nz]
    h = pl.program_id(0)

    @pl.when(h == 0)
    def _():
        acc[...] = jnp.zeros_like(acc)

    src = outs[0].shape[0]
    c = c_ref[0, 0:1, :].astype(BF16)
    q = jnp.concatenate([r[:rows, :] for r in qs], axis=0)
    g = jnp.concatenate([r[...] for r in gs], axis=0)
    for z in range(nz):
        part = slice(z * src, (z + 1) * src)
        acc[part, :HD] += dot(ds_ref[0, part, :] * c, q, 1, 0)
        acc[part, HD:] += dot(p_ref[0, part, :] * c, g, 1, 0)

    @pl.when(h == pl.num_programs(0) - 1)
    def _():
        for z in range(nz):
            part = slice(z * src, (z + 1) * src)
            outs[z][:, :HD] = (acc[part, :HD] * scaling).astype(BF16)
            outs[z][:, HD:] = acc[part, HD:].astype(BF16)


def local(target, source, target_gain, source_gain, w_query, w_key, w_value, attended, d_attended):
    sp, tp = lax.axis_size("sp"), lax.axis_size("tp")
    me, mt = lax.axis_index("sp"), lax.axis_index("tp")
    rows, dim = target.shape
    srows = source.shape[0]
    width = w_query.shape[1]
    heads = width // HD
    group = tp // KVH
    nb = min(4, sp)
    nz = sp // nb
    scaling = HD ** (-0.5)
    kv_index = mt // group
    dblk = dim // sp

    normed_source = norm_rows(source, source_gain)
    key_all = dot(normed_source, w_key, 1, 0).astype(BF16)
    value_all = dot(normed_source, w_value, 1, 0).astype(BF16)
    by_head = []
    for r in range(KVH):
        start = (kv_index ^ r) * HD
        by_head.append(
            jnp.concatenate(
                [
                    lax.dynamic_slice_in_dim(key_all, start, HD, 1),
                    lax.dynamic_slice_in_dim(value_all, start, HD, 1),
                ],
                axis=1,
            )
        )
    kv_tp = [by_head[0]] + [swap(by_head[d // group], "tp", d) for d in range(1, tp)]
    kv_own = jnp.concatenate(kv_tp, axis=0)
    kvs = [kv_own] + [swap(kv_own, "sp", k * nb) for k in range(1, nz)]

    normed_target = norm_rows(target, target_gain)
    query = dot(normed_target, w_query, 1, 0).astype(BF16)
    delta = jnp.sum(
        (d_attended.astype(F32) * attended.astype(F32)).reshape(rows, heads, HD), axis=-1
    ).astype(BF16)
    delta_row = jnp.pad(delta, ((0, HD - rows), (0, 0))).T.reshape(1, width)
    q_ext = jnp.concatenate([query, delta_row, jnp.zeros((15, width), BF16)], axis=0)
    gs = [d_attended] + [swap(d_attended, "sp", k) for k in range(1, nb)]
    qs = [q_ext] + [swap(q_ext, "sp", k) for k in range(1, nb)]

    held, _ = lax.optimization_barrier((w_query, kvs[-1]))
    wqs = [w_query] + [swap(held, "tp", d) for d in range(1, tp)]

    cols = [
        lax.dynamic_slice_in_dim(normed_target, (me ^ j) * dblk, dblk, 1) for j in range(sp)
    ]
    half = nb // 2
    near = [j for j in range(sp) if (j & half) == 0]
    nt_own = jnp.concatenate([cols[j] for j in near], axis=1)
    nt_far = swap(jnp.concatenate([cols[j ^ half] for j in near], axis=1), "sp", half)
    nt_cat = jnp.concatenate([nt_own, nt_far], axis=0)

    src = kv_own.shape[0]
    total_src = nz * src
    trows = nb * rows
    qspec = pl.BlockSpec((rows + 16, HD), lambda h: (0, h))
    gspec = pl.BlockSpec((rows, HD), lambda h: (0, h))
    kvspec = pl.BlockSpec((src, 2 * HD), lambda h: (0, 0))
    pspec = pl.BlockSpec((1, total_src, trows), lambda h: (h, 0, 0))
    stspec = pl.BlockSpec((1, 8, trows), lambda h: (h, 0, 0))
    dqspec = pl.BlockSpec((1, HD, trows), lambda h: (h, 0, 0))
    pshape = jax.ShapeDtypeStruct((heads, total_src, trows), BF16)
    stshape = jax.ShapeDtypeStruct((heads, 8, trows), F32)
    flops = 2 * heads * total_src * trows * HD
    probs, stats = pl.pallas_call(
        functools.partial(scores_kernel, nz, nb, rows, scaling),
        grid=(heads,),
        in_specs=[kvspec] * nz + [qspec] * nb,
        out_specs=[pspec, stspec],
        out_shape=[pshape, stshape],
        compiler_params=params(),
        cost_estimate=pl.CostEstimate(flops=2 * flops, bytes_accessed=6 << 20, transcendentals=0),
    )(*kvs, *qs)
    sts = [stats] + [swap(stats, "sp", k) for k in range(1, nb)]
    d_scores, dq_t = pl.pallas_call(
        functools.partial(grads_kernel, nz, nb, rows),
        grid=(heads,),
        in_specs=[kvspec] * nz + [qspec] * nb + [gspec] * nb + [pspec],
        out_specs=[pspec, dqspec],
        out_shape=[pshape, jax.ShapeDtypeStruct((heads, HD, trows), F32)],
        compiler_params=params(),
        cost_estimate=pl.CostEstimate(flops=3 * flops, bytes_accessed=10 << 20, transcendentals=0),
    )(*kvs, *qs, *gs, probs)
    whole = lambda shape: pl.BlockSpec(shape, lambda i: (0,) * len(shape))
    coef, *dqs = pl.pallas_call(
        functools.partial(scale_kernel, nb, rows, heads, scaling),
        grid=(1,),
        in_specs=[whole((heads, 8, trows))] * nb + [whole((heads, HD, trows))],
        out_specs=[whole((heads, 8, trows))] + [whole((rows, width))] * nb,
        out_shape=[stshape] + [jax.ShapeDtypeStruct((rows, width), BF16)] * nb,
        compiler_params=params(),
        cost_estimate=pl.CostEstimate(flops=1 << 26, bytes_accessed=2 << 20, transcendentals=0),
    )(*sts, dq_t)
    dkvs = pl.pallas_call(
        functools.partial(keyvalue_kernel, nz, nb, rows, scaling),
        grid=(heads,),
        in_specs=[qspec] * nb + [gspec] * nb + [stspec, pspec, pspec],
        out_specs=[kvspec] * nz,
        out_shape=[jax.ShapeDtypeStruct((src, 2 * HD), BF16)] * nz,
        scratch_shapes=[pltpu.VMEM((total_src, 2 * HD), F32)],
        compiler_params=params(),
        cost_estimate=pl.CostEstimate(flops=3 * flops, bytes_accessed=10 << 20, transcendentals=0),
    )(*qs, *gs, coef, probs, d_scores)

    sent = jnp.concatenate([dqs[1], dqs[half + 1]], axis=0)
    kept = jnp.concatenate([dqs[0], dqs[half]], axis=0)
    pair_sum = kept.astype(F32) + swap(sent, "sp", 1).astype(F32)
    pair_b = pair_sum.astype(BF16)
    other = swap(pair_b, "sp", half)
    other = jnp.concatenate([other[rows:], other[:rows]], axis=0)
    d_query2 = (pair_b.astype(F32) + other.astype(F32)).astype(BF16)

    partial = dot(nt_cat, d_query2, 0, 0).astype(BF16).reshape(nz, 2, dblk, width)
    mine = partial[:, 0].astype(F32) + swap(partial[:, 1], "sp", 1).astype(F32)
    mine_b = mine.astype(BF16)
    d_w_query = mine[0]
    for k in range(1, nz):
        d_w_query = d_w_query + swap(mine_b[k], "sp", k * nb).astype(F32)

    dq_own = d_query2[:rows]
    d_normed = dot(dq_own, wqs[0], 1, 1)
    for d in range(1, tp):
        d_normed = d_normed + dot(swap(dq_own, "tp", d), wqs[d], 1, 1)
    d_target = norm_back(target, target_gain, d_normed).astype(BF16)

    dkv = dkvs[0].astype(F32)
    for k in range(1, nz):
        dkv = dkv + swap(dkvs[k], "sp", k * nb).astype(F32)
    dkv = dkv.astype(BF16).reshape(tp, srows, 2 * HD)
    relative = [None] * KVH
    for d in range(tp):
        block = dkv[0] if d == 0 else swap(dkv[d], "tp", d)
        block = block.astype(F32)
        r = d // group
        relative[r] = block if relative[r] is None else relative[r] + block
    stacked = jnp.stack([x.astype(BF16) for x in relative], axis=0)
    absolute = [lax.dynamic_index_in_dim(stacked, kv_index ^ a, 0, False) for a in range(KVH)]
    d_key = jnp.concatenate([x[:, :HD] for x in absolute], axis=1)
    d_value = jnp.concatenate([x[:, HD:] for x in absolute], axis=1)
    d_normed_source = dot(d_key, w_key, 1, 1) + dot(d_value, w_value, 1, 1)
    d_source = norm_back(source, source_gain, d_normed_source)
    return (d_target, d_source, d_w_query)


def solution(mesh):
    return jax.shard_map(
        local,
        mesh=mesh,
        in_specs=(
            P("sp", None),
            P(("sp", "tp"), None),
            P(),
            P(),
            P(None, "tp"),
            P(),
            P(),
            P("sp", "tp"),
            P("sp", "tp"),
        ),
        out_specs=(P("sp", None), P(("sp", "tp"), None), P("sp", "tp")),
        check_vma=False,
    )
```

```python
import functools

import jax
import jax.numpy as jnp
from jax import lax
from jax.experimental import pallas as pl
from jax.experimental.pallas import tpu as pltpu
from jax.sharding import PartitionSpec as P


KVH = 2
HD = 128
EPS = 1e-06
LOG2E = 1.4426950408889634


F32 = jnp.float32
BF16 = jnp.bfloat16


def swap(x, axis, k):
    n = lax.axis_size(axis)
    return lax.ppermute(x, axis, [(i, i ^ k) for i in range(n)])


def norm_parts(matrix):
    widened = matrix.astype(F32)
    inverse = lax.rsqrt(jnp.mean(widened * widened, axis=-1, keepdims=True) + EPS)
    return widened, inverse


def norm_back(matrix, gain_vector, cotangent):
    widened, inverse = norm_parts(matrix)
    scaled = cotangent * gain_vector
    inner = jnp.mean(widened * scaled, axis=-1, keepdims=True)
    return inverse * scaled - widened * (inverse * inverse * inverse * inner)


def dot(a, b, ca, cb):
    return lax.dot_general(a, b, (((ca,), (cb,)), ((), ())), preferred_element_type=F32)


def params(mb=20):
    return pltpu.CompilerParams(
        vmem_limit_bytes=mb * 1024 * 1024, dimension_semantics=("arbitrary",)
    )


def normed(x, gain):
    wide = x.astype(F32)
    inverse = lax.rsqrt(jnp.mean(wide * wide, axis=-1, keepdims=True) + EPS)
    return (wide * inverse * gain).astype(BF16)


def source_kernel(steps, idx_ref, x_ref, g_ref, wk_ref, wv_ref, o_ref, n_ref, k_acc, v_acc):
    i = pl.program_id(0)
    chunk = wk_ref.shape[0]

    @pl.when(i == 0)
    def _():
        n_ref[...] = normed(x_ref[...], g_ref[...])
        k_acc[...] = jnp.zeros_like(k_acc)
        v_acc[...] = jnp.zeros_like(v_acc)

    for s in range(steps):

        @pl.when(i == s)
        def _():
            part = n_ref[:, s * chunk : (s + 1) * chunk]
            k_acc[...] += dot(part, wk_ref[...], 1, 0)
            v_acc[...] += dot(part, wv_ref[...], 1, 0)

    @pl.when(i == steps - 1)
    def _():
        for a in range(KVH):
            r = a ^ idx_ref[0]
            o_ref[r, :, :HD] = k_acc[:, a * HD : (a + 1) * HD].astype(BF16)
            o_ref[r, :, HD:] = v_acc[:, a * HD : (a + 1) * HD].astype(BF16)


def target_kernel(steps, sp, half, idx_ref, x_ref, g_ref, wq_ref, at_ref, da_ref, q_ref, near_ref, far_ref, n_ref, t_ref, q_acc):
    i = pl.program_id(0)
    chunk = wq_ref.shape[0]
    rows = x_ref.shape[0]
    dblk = t_ref.shape[0] // sp

    @pl.when(i == 0)
    def _():
        n_ref[...] = normed(x_ref[...], g_ref[...])
        q_acc[...] = jnp.zeros_like(q_acc)

    for s in range(steps):

        @pl.when(i == s)
        def _():
            part = n_ref[:, s * chunk : (s + 1) * chunk]
            q_acc[...] += dot(part, wq_ref[...], 1, 0)
            t_ref[s * chunk : (s + 1) * chunk, :] = part.T

    @pl.when(i == steps - 1)
    def _():
        q_ref[:rows, :] = q_acc[...].astype(BF16)
        prod = da_ref[...].astype(F32) * at_ref[...].astype(F32)
        q_ref[rows:, :] = jnp.zeros_like(q_ref[rows:, :])
        for h in range(prod.shape[1] // HD):
            d = jnp.sum(prod[:, h * HD : (h + 1) * HD].T, axis=0, keepdims=True)
            q_ref[rows : rows + 1, h * HD : h * HD + rows] = d.astype(BF16)
        me = idx_ref[0]
        n = 0
        for j in range(sp):
            if j & half:
                continue
            here = pl.multiple_of((me ^ j) * dblk, dblk)
            there = pl.multiple_of((me ^ j ^ half) * dblk, dblk)
            near_ref[n * dblk : (n + 1) * dblk, :] = t_ref[pl.ds(here, dblk), :]
            far_ref[n * dblk : (n + 1) * dblk, :] = t_ref[pl.ds(there, dblk), :]
            n += 1


def scores_kernel(nz, nb, rows, scaling, *refs):
    kvs, qs, (p_ref, st_ref) = refs[:nz], refs[nz : nz + nb], refs[nz + nb :]
    src = kvs[0].shape[0]
    for pair in range(nb // 2):
        q = jnp.concatenate([qs[2 * pair][:rows, :], qs[2 * pair + 1][:rows, :]], axis=0)
        cols = slice(pair * 2 * rows, (pair + 1) * 2 * rows)
        parts = [dot(kv[:, :HD], q, 1, 1) for kv in kvs]
        top = functools.reduce(
            jnp.maximum, [jnp.max(s, axis=0, keepdims=True) for s in parts]
        )
        total = jnp.zeros_like(top)
        for z, s in enumerate(parts):
            p = jnp.exp2((s - top) * (scaling * LOG2E))
            total = total + jnp.sum(p, axis=0, keepdims=True)
            p_ref[0, z * src : (z + 1) * src, cols] = p.astype(BF16)
        st_ref[0, 0:1, cols] = top * (scaling * LOG2E)
        st_ref[0, 1:2, cols] = total


def grads_kernel(nz, nb, rows, *refs):
    kvs, qs, gs = refs[:nz], refs[nz : nz + nb], refs[nz + nb : nz + 2 * nb]
    p_ref, ds_ref, dq_ref = refs[nz + 2 * nb :]
    src = kvs[0].shape[0]
    for pair in range(nb // 2):
        a, b = 2 * pair, 2 * pair + 1
        g = jnp.concatenate([gs[a][...], gs[b][...]], axis=0)
        delta = jnp.concatenate(
            [qs[a][rows : rows + 1, :], qs[b][rows : rows + 1, :]], axis=1
        ).astype(F32)
        cols = slice(pair * 2 * rows, (pair + 1) * 2 * rows)
        acc = None
        for z, kv in enumerate(kvs):
            dw = dot(kv[:, HD:], g, 1, 1)
            p = p_ref[0, z * src : (z + 1) * src, cols].astype(F32)
            ds = (p * (dw - delta)).astype(BF16)
            ds_ref[0, z * src : (z + 1) * src, cols] = ds
            part = dot(kv[:, :HD], ds, 0, 0)
            acc = part if acc is None else acc + part
        dq_ref[0, :, cols] = acc


def scale_kernel(nb, rows, heads, scaling, *refs):
    sts = refs[:nb]
    dq_ref, c_ref = refs[nb], refs[nb + 1]
    sent_ref, kept_ref = refs[nb + 2 :]
    places = [(kept_ref, 0), (sent_ref, 0)]
    if nb > 2:
        places = [(kept_ref, 0), (sent_ref, 0), (kept_ref, 1), (sent_ref, 1)]
    for h in range(heads):
        own_top = sts[0][h, 0:1, :]
        tops, sums = [own_top], [sts[0][h, 1:2, :]]
        for k in range(1, nb):
            order = [j ^ k for j in range(nb)]
            tops.append(
                jnp.concatenate([sts[k][h, 0:1, o * rows : (o + 1) * rows] for o in order], axis=1)
            )
            sums.append(
                jnp.concatenate([sts[k][h, 1:2, o * rows : (o + 1) * rows] for o in order], axis=1)
            )
        top = functools.reduce(jnp.maximum, tops)
        total = sum(s * jnp.exp2(t - top) for t, s in zip(tops, sums))
        c = jnp.exp2(own_top - top) / total
        c_ref[h, 0:1, :] = c
        for k in range(nb):
            part = slice(k * rows, (k + 1) * rows)
            block = dq_ref[h, :, part] * (c[:, part] * scaling)
            ref, spot = places[k]
            ref[spot * rows : (spot + 1) * rows, h * HD : (h + 1) * HD] = block.T.astype(ref.dtype)


def keyvalue_kernel(nz, nb, rows, scaling, *refs):
    qs, gs = refs[:nb], refs[nb : 2 * nb]
    c_ref, p_ref, ds_ref = refs[2 * nb : 2 * nb + 3]
    outs = refs[2 * nb + 3 : 2 * nb + 3 + nz]
    acc = refs[2 * nb + 3 + nz]
    h = pl.program_id(0)

    @pl.when(h == 0)
    def _():
        acc[...] = jnp.zeros_like(acc)

    src = outs[0].shape[0]
    c = c_ref[0, 0:1, :].astype(BF16)
    q = jnp.concatenate([r[:rows, :] for r in qs], axis=0)
    g = jnp.concatenate([r[...] for r in gs], axis=0)
    for z in range(nz):
        part = slice(z * src, (z + 1) * src)
        acc[part, :HD] += dot(ds_ref[0, part, :] * c, q, 1, 0)
        acc[part, HD:] += dot(p_ref[0, part, :] * c, g, 1, 0)

    @pl.when(h == pl.num_programs(0) - 1)
    def _():
        for z in range(nz):
            part = slice(z * src, (z + 1) * src)
            outs[z][:, :HD] = (acc[part, :HD] * scaling).astype(BF16)
            outs[z][:, HD:] = acc[part, HD:].astype(BF16)


def first_kernel(nz, dblk, rows, pair_ref, other_ref, near_ref, far_ref, dq_ref, o_ref):
    dq_ref[:rows, :] = (pair_ref[:rows, :].astype(F32) + other_ref[rows:, :].astype(F32)).astype(BF16)
    dq_ref[rows:, :] = (pair_ref[rows:, :].astype(F32) + other_ref[:rows, :].astype(F32)).astype(BF16)
    dq = dq_ref[...]
    for k in range(nz):
        at = slice((2 * k + 1) * dblk, (2 * k + 2) * dblk)
        left = jnp.concatenate([near_ref[at, :], far_ref[at, :]], axis=1)
        o_ref[k * dblk : (k + 1) * dblk, :] = dot(left, dq, 1, 0).astype(BF16)


def second_kernel(nz, dblk, dq_ref, near_ref, far_ref, got_ref, *outs):
    dq = dq_ref[...]
    for k in range(nz):
        at = slice(2 * k * dblk, (2 * k + 1) * dblk)
        left = jnp.concatenate([near_ref[at, :], far_ref[at, :]], axis=1)
        total = dot(left, dq, 1, 0) + got_ref[k * dblk : (k + 1) * dblk, :].astype(F32)
        outs[k][...] = total.astype(outs[k].dtype)


def whole(shape):
    return pl.BlockSpec(shape, lambda *_: (0,) * len(shape))


def estimate(flops, mib):
    return pl.CostEstimate(flops=flops, bytes_accessed=mib << 20, transcendentals=0)


def local(target, source, target_gain, source_gain, w_query, w_key, w_value, attended, d_attended):
    sp, tp = lax.axis_size("sp"), lax.axis_size("tp")
    me, mt = lax.axis_index("sp"), lax.axis_index("tp")
    rows, dim = target.shape
    srows = source.shape[0]
    width = w_query.shape[1]
    heads = width // HD
    group = tp // KVH
    nb = min(4, sp)
    nz = sp // nb
    half = nb // 2
    scaling = HD ** (-0.5)
    kv_index = mt // group
    dblk = dim // sp
    steps = 4
    chunk = dim // steps

    kvw = KVH * HD
    by_head = pl.pallas_call(
        functools.partial(source_kernel, steps),
        grid_spec=pltpu.PrefetchScalarGridSpec(
            num_scalar_prefetch=1,
            grid=(steps,),
            in_specs=[
                whole((srows, dim)),
                whole((1, dim)),
                pl.BlockSpec((chunk, kvw), lambda i, *_: (i, 0)),
                pl.BlockSpec((chunk, kvw), lambda i, *_: (i, 0)),
            ],
            out_specs=whole((KVH, srows, 2 * HD)),
            scratch_shapes=[
                pltpu.VMEM((srows, dim), BF16),
                pltpu.VMEM((srows, kvw), F32),
                pltpu.VMEM((srows, kvw), F32),
            ],
        ),
        out_shape=jax.ShapeDtypeStruct((KVH, srows, 2 * HD), BF16),
        compiler_params=params(),
        cost_estimate=estimate(4 * srows * dim * kvw, 3),
    )(kv_index.astype(jnp.int32).reshape(1), source, source_gain.reshape(1, dim), w_key, w_value)
    kv_tp = [by_head[0]] + [swap(by_head[d // group], "tp", d) for d in range(1, tp)]
    kv_own = jnp.concatenate(kv_tp, axis=0)
    kvs = [kv_own] + [swap(kv_own, "sp", k * nb) for k in range(1, nz)]

    target_b, d_attended_b, _ = lax.optimization_barrier((target, d_attended, by_head))
    near_rows = dim // 2
    q_ext, near, far = pl.pallas_call(
        functools.partial(target_kernel, steps, sp, half),
        grid_spec=pltpu.PrefetchScalarGridSpec(
            num_scalar_prefetch=1,
            grid=(steps,),
            in_specs=[
                whole((rows, dim)),
                whole((1, dim)),
                pl.BlockSpec((chunk, width), lambda i, *_: (i, 0)),
                whole((rows, width)),
                whole((rows, width)),
            ],
            out_specs=[whole((rows + 16, width)), whole((near_rows, rows)), whole((near_rows, rows))],
            scratch_shapes=[
                pltpu.VMEM((rows, dim), BF16),
                pltpu.VMEM((dim, rows), BF16),
                pltpu.VMEM((rows, width), F32),
            ],
        ),
        out_shape=[
            jax.ShapeDtypeStruct((rows + 16, width), BF16),
            jax.ShapeDtypeStruct((near_rows, rows), BF16),
            jax.ShapeDtypeStruct((near_rows, rows), BF16),
        ],
        compiler_params=params(),
        cost_estimate=estimate(2 * rows * dim * width, 4),
    )(me.astype(jnp.int32).reshape(1), target_b, target_gain.reshape(1, dim), w_query, attended, d_attended_b)
    gs = [d_attended] + [swap(d_attended_b, "sp", k) for k in range(1, nb)]
    qs = [q_ext] + [swap(q_ext, "sp", k) for k in range(1, nb)]
    far = swap(far, "sp", half)

    held, _ = lax.optimization_barrier((w_query, kv_own))
    wqs = [w_query] + [swap(held, "tp", d) for d in range(1, tp)]

    src = kv_own.shape[0]
    total_src = nz * src
    trows = nb * rows
    qspec = pl.BlockSpec((rows + 16, HD), lambda h: (0, h))
    gspec = pl.BlockSpec((rows, HD), lambda h: (0, h))
    kvspec = pl.BlockSpec((src, 2 * HD), lambda h: (0, 0))
    pspec = pl.BlockSpec((1, total_src, trows), lambda h: (h, 0, 0))
    stspec = pl.BlockSpec((1, 8, trows), lambda h: (h, 0, 0))
    dqspec = pl.BlockSpec((1, HD, trows), lambda h: (h, 0, 0))
    pshape = jax.ShapeDtypeStruct((heads, total_src, trows), BF16)
    stshape = jax.ShapeDtypeStruct((heads, 8, trows), F32)
    flops = 2 * heads * total_src * trows * HD
    probs, stats = pl.pallas_call(
        functools.partial(scores_kernel, nz, nb, rows, scaling),
        grid=(heads,),
        in_specs=[kvspec] * nz + [qspec] * nb,
        out_specs=[pspec, stspec],
        out_shape=[pshape, stshape],
        compiler_params=params(),
        cost_estimate=estimate(2 * flops, 6),
    )(*kvs, *qs)
    sts = [stats] + [swap(stats, "sp", k) for k in range(1, nb)]
    d_scores, dq_t = pl.pallas_call(
        functools.partial(grads_kernel, nz, nb, rows),
        grid=(heads,),
        in_specs=[kvspec] * nz + [qspec] * nb + [gspec] * nb + [pspec],
        out_specs=[pspec, dqspec],
        out_shape=[pshape, jax.ShapeDtypeStruct((heads, HD, trows), F32)],
        compiler_params=params(),
        cost_estimate=estimate(3 * flops, 10),
    )(*kvs, *qs, *gs, probs)
    coef, sent, kept = pl.pallas_call(
        functools.partial(scale_kernel, nb, rows, heads, scaling),
        grid=(1,),
        in_specs=[whole((heads, 8, trows))] * nb + [whole((heads, HD, trows))],
        out_specs=[whole((heads, 8, trows))] + [whole((2 * rows, width))] * 2,
        out_shape=[
            stshape,
            jax.ShapeDtypeStruct((2 * rows, width), BF16),
            jax.ShapeDtypeStruct((2 * rows, width), F32),
        ],
        compiler_params=params(),
        cost_estimate=estimate(1 << 26, 2),
    )(*sts, dq_t)
    dkvs = pl.pallas_call(
        functools.partial(keyvalue_kernel, nz, nb, rows, scaling),
        grid=(heads,),
        in_specs=[qspec] * nb + [gspec] * nb + [stspec, pspec, pspec],
        out_specs=[kvspec] * nz,
        out_shape=[jax.ShapeDtypeStruct((src, 2 * HD), BF16)] * nz,
        scratch_shapes=[pltpu.VMEM((total_src, 2 * HD), F32)],
        compiler_params=params(),
        cost_estimate=estimate(3 * flops, 10),
    )(*qs, *gs, coef, probs, d_scores)

    pair_b = (kept + swap(sent, "sp", 1).astype(F32)).astype(BF16)
    other = swap(pair_b, "sp", half)

    d_query2, partial = pl.pallas_call(
        functools.partial(first_kernel, nz, dblk, rows),
        grid=(1,),
        in_specs=[whole((2 * rows, width))] * 2 + [whole((near_rows, rows))] * 2,
        out_specs=[whole((2 * rows, width)), whole((nz * dblk, width))],
        out_shape=[
            jax.ShapeDtypeStruct((2 * rows, width), BF16),
            jax.ShapeDtypeStruct((nz * dblk, width), BF16),
        ],
        compiler_params=params(),
        cost_estimate=estimate(4 * rows * nz * dblk * width, 3),
    )(pair_b, other, near, far)
    got = swap(partial, "sp", 1)
    mine = pl.pallas_call(
        functools.partial(second_kernel, nz, dblk),
        grid=(1,),
        in_specs=[whole((2 * rows, width))] + [whole((near_rows, rows))] * 2 + [whole((nz * dblk, width))],
        out_specs=[whole((dblk, width))] * nz,
        out_shape=[jax.ShapeDtypeStruct((dblk, width), F32)]
        + [jax.ShapeDtypeStruct((dblk, width), BF16)] * (nz - 1),
        compiler_params=params(),
        cost_estimate=estimate(4 * rows * nz * dblk * width, 3),
    )(d_query2, near, far, got)
    d_w_query = mine[0]
    for k in range(1, nz):
        d_w_query = d_w_query + swap(mine[k], "sp", k * nb).astype(F32)

    dq_own = d_query2[:rows]
    dqs = [dq_own] + [swap(dq_own, "tp", d) for d in range(1, tp)]
    d_normed = dot(dqs[0], wqs[0], 1, 1)
    for d in range(1, tp):
        d_normed = d_normed + dot(dqs[d], wqs[d], 1, 1)
    d_target = norm_back(target, target_gain, d_normed).astype(BF16)

    dkv = dkvs[0].astype(F32)
    for k in range(1, nz):
        dkv = dkv + swap(dkvs[k], "sp", k * nb).astype(F32)
    dkv = dkv.astype(BF16).reshape(tp, srows, 2 * HD)
    relative = [None] * KVH
    for d in range(tp):
        block = dkv[0] if d == 0 else swap(dkv[d], "tp", d)
        block = block.astype(F32)
        r = d // group
        relative[r] = block if relative[r] is None else relative[r] + block
    stacked = jnp.stack([x.astype(BF16) for x in relative], axis=0)
    absolute = [lax.dynamic_index_in_dim(stacked, kv_index ^ a, 0, False) for a in range(KVH)]
    d_key = jnp.concatenate([x[:, :HD] for x in absolute], axis=1)
    d_value = jnp.concatenate([x[:, HD:] for x in absolute], axis=1)
    d_normed_source = dot(d_key, w_key, 1, 1) + dot(d_value, w_value, 1, 1)
    d_source = norm_back(source, source_gain, d_normed_source)
    return (d_target, d_source, d_w_query)


def solution(mesh):
    return jax.shard_map(
        local,
        mesh=mesh,
        in_specs=(
            P("sp", None),
            P(("sp", "tp"), None),
            P(),
            P(),
            P(None, "tp"),
            P(),
            P(),
            P("sp", "tp"),
            P("sp", "tp"),
        ),
        out_specs=(P("sp", None), P(("sp", "tp"), None), P("sp", "tp")),
        check_vma=False,
    )
```

```python
import functools

import jax
import jax.numpy as jnp
from jax import lax
from jax.experimental import pallas as pl
from jax.experimental.pallas import tpu as pltpu
from jax.sharding import PartitionSpec as P


KVH = 2
HD = 128
EPS = 1e-06
LOG2E = 1.4426950408889634
FRONT_MIB = 60


F32 = jnp.float32
BF16 = jnp.bfloat16


def swap(x, axis, k):
    n = lax.axis_size(axis)
    return lax.ppermute(x, axis, [(i, i ^ k) for i in range(n)])


def dot(a, b, ca, cb):
    return lax.dot_general(a, b, (((ca,), (cb,)), ((), ())), preferred_element_type=F32)


def normed(x, gain):
    wide = x.astype(F32)
    inverse = lax.rsqrt(jnp.mean(wide * wide, axis=-1, keepdims=True) + EPS)
    return (wide * inverse * gain).astype(BF16)


def norm_back(x, gain, cotangent):
    wide = x.astype(F32)
    inverse = lax.rsqrt(jnp.mean(wide * wide, axis=-1, keepdims=True) + EPS)
    scaled = cotangent * gain
    inner = jnp.mean(wide * scaled, axis=-1, keepdims=True)
    return inverse * scaled - wide * (inverse * inverse * inverse * inner)


def chunk_copy(src, dst, sem, s, size):
    at = pl.ds(s * size, size)
    return pltpu.make_async_copy(src.at[at, :], dst.at[at, :], sem.at[s])


def source_kernel(steps, kv_ref, x_any, g_any, wk_any, wv_any, *refs):
    outs = refs[:KVH]
    x_ref, g_ref, wk_ref, wv_ref, k_ref, v_ref, sem, k_sem, v_sem = refs[KVH:]
    chunk = wk_ref.shape[0] // steps
    first = [
        pltpu.make_async_copy(x_any, x_ref, sem.at[0]),
        pltpu.make_async_copy(g_any, g_ref, sem.at[1]),
    ]
    wks = [chunk_copy(wk_any, wk_ref, k_sem, s, chunk) for s in range(steps)]
    wvs = [chunk_copy(wv_any, wv_ref, v_sem, s, chunk) for s in range(steps)]
    for copy in first:
        copy.start()
    for s in range(steps):
        wks[s].start()
        wvs[s].start()
    for copy in first:
        copy.wait()
    x_ref[...] = normed(x_ref[...], g_ref[...])
    k_acc, v_acc = None, None
    for s in range(steps):
        part = slice(s * chunk, (s + 1) * chunk)
        wks[s].wait()
        k = dot(x_ref[:, part], wk_ref[part, :], 1, 0)
        wvs[s].wait()
        v = dot(x_ref[:, part], wv_ref[part, :], 1, 0)
        k_acc = k if k_acc is None else k_acc + k
        v_acc = v if v_acc is None else v_acc + v
    k_ref[...] = k_acc.astype(BF16)
    v_ref[...] = v_acc.astype(BF16)
    for r in range(KVH):
        at = pl.ds(pl.multiple_of((kv_ref[0] ^ r) * HD, HD), HD)
        outs[r][:, :HD] = k_ref[:, at]
        outs[r][:, HD:] = v_ref[:, at]


def target_kernel(steps, sp, half, me_ref, x_any, g_any, wq_any, at_any, da_any, *refs):
    q_ref, near_ref, far_ref = refs[:3]
    x_ref, g_ref, wq_ref, at_ref, da_ref, nt_ref, sem, q_sem = refs[3:]
    dim = wq_ref.shape[0]
    chunk = dim // steps
    rows = x_ref.shape[0]
    dblk = dim // sp
    pairs = ((x_any, x_ref), (g_any, g_ref), (da_any, da_ref), (at_any, at_ref))
    copies = [pltpu.make_async_copy(a, b, sem.at[i]) for i, (a, b) in enumerate(pairs)]
    wqs = [chunk_copy(wq_any, wq_ref, q_sem, s, chunk) for s in range(steps)]
    for copy in copies + wqs:
        copy.start()
    for copy in copies[:2]:
        copy.wait()
    x_ref[...] = normed(x_ref[...], g_ref[...])
    for s in range(steps):
        part = slice(s * chunk, (s + 1) * chunk)
        nt_ref[part, :] = x_ref[:, part].T
    for copy in copies[2:]:
        copy.wait()
    prod = da_ref[...].astype(F32) * at_ref[...].astype(F32)
    q_ref[rows:, :] = jnp.zeros_like(q_ref[rows:, :])
    for h in range(prod.shape[1] // HD):
        d = jnp.sum(prod[:, h * HD : (h + 1) * HD].T, axis=0, keepdims=True)
        q_ref[rows : rows + 1, h * HD : h * HD + rows] = d.astype(BF16)
    me = me_ref[0]
    n = 0
    for j in range(sp):
        if j & half:
            continue
        here = pl.multiple_of((me ^ j) * dblk, dblk)
        there = pl.multiple_of((me ^ j ^ half) * dblk, dblk)
        near_ref[n * dblk : (n + 1) * dblk, :] = nt_ref[pl.ds(here, dblk), :]
        far_ref[n * dblk : (n + 1) * dblk, :] = nt_ref[pl.ds(there, dblk), :]
        n += 1
    q_acc = None
    for s in range(steps):
        part = slice(s * chunk, (s + 1) * chunk)
        wqs[s].wait()
        q = dot(x_ref[:, part], wq_ref[part, :], 1, 0)
        q_acc = q if q_acc is None else q_acc + q
    q_ref[:rows, :] = q_acc.astype(BF16)


def scores_kernel(nk, nb, rows, scaling, *refs):
    kvs, qs = refs[:nk], refs[nk : nk + nb]
    p_ref, st_ref, k_ref, v_ref, kt_ref = refs[nk + nb :]
    at = 0
    for kv in kvs:
        size = kv.shape[0]
        k_ref[at : at + size, :] = kv[:, :HD]
        v_ref[at : at + size, :] = kv[:, HD:]
        at += size
    kt_ref[...] = k_ref[...].T
    for h in range(p_ref.shape[0]):
        lanes = slice(h * HD, (h + 1) * HD)
        for pair in range(nb // 2):
            q = jnp.concatenate(
                [qs[2 * pair + i][:rows, lanes] for i in range(2)], axis=0
            )
            cols = slice(pair * 2 * rows, (pair + 1) * 2 * rows)
            s = dot(k_ref[...], q, 1, 1)
            top = jnp.max(s, axis=0, keepdims=True)
            p = jnp.exp2((s - top) * (scaling * LOG2E))
            p_ref[h, :, cols] = p.astype(BF16)
            st_ref[h, 0:1, cols] = top * (scaling * LOG2E)
            st_ref[h, 1:2, cols] = jnp.sum(p, axis=0, keepdims=True)


def grads_kernel(nb, rows, v_ref, kt_ref, p_ref, *refs):
    qs, gs = refs[:nb], refs[nb : 2 * nb]
    ds_ref, dq_ref = refs[2 * nb :]
    for h in range(p_ref.shape[0]):
        lanes = slice(h * HD, (h + 1) * HD)
        for pair in range(nb // 2):
            both = (2 * pair, 2 * pair + 1)
            g = jnp.concatenate([gs[i][:, lanes] for i in both], axis=0)
            delta = jnp.concatenate([qs[i][rows : rows + 1, lanes] for i in both], axis=1).astype(F32)
            cols = slice(pair * 2 * rows, (pair + 1) * 2 * rows)
            dw = dot(v_ref[...], g, 1, 1)
            ds = (p_ref[h, :, cols].astype(F32) * (dw - delta)).astype(BF16)
            ds_ref[h, :, cols] = ds
            dq_ref[h, :, cols] = dot(kt_ref[...], ds, 1, 0)


def lse_kernel(heads, a_ref, b_ref, o_ref):
    o_ref[...] = jnp.zeros_like(o_ref)
    for h in range(heads):
        ta, tb = a_ref[h, 0:1, :], b_ref[h, 0:1, :]
        top = jnp.maximum(ta, tb)
        total = a_ref[h, 1:2, :] * jnp.exp2(ta - top) + b_ref[h, 1:2, :] * jnp.exp2(tb - top)
        o_ref[h : h + 1, :] = top
        o_ref[heads + h : heads + h + 1, :] = total


def scale_kernel(nb, rows, heads, scaling, *refs):
    own_a, own_b = refs[:2]
    sts = refs[2 : nb + 1]
    dqa_ref, dqb_ref, c_ref, sent_ref, kept_ref = refs[nb + 1 :]
    places = [(kept_ref, 0), (sent_ref, 0), (kept_ref, 1), (sent_ref, 1)]
    for h in range(heads):
        tops = [own_a[h, 0:1, :], own_b[h, 0:1, :]]
        sums = [own_a[h, 1:2, :], own_b[h, 1:2, :]]
        for k in range(1, nb):
            order = [slice((j ^ k) * rows, (j ^ k) * rows + rows) for j in range(nb)]
            st = sts[k - 1]
            tops.append(jnp.concatenate([st[h : h + 1, o] for o in order], axis=1))
            low = heads + h
            sums.append(jnp.concatenate([st[low : low + 1, o] for o in order], axis=1))
        top = functools.reduce(jnp.maximum, tops)
        total = sum(s * jnp.exp2(t - top) for t, s in zip(tops, sums))
        ca = jnp.exp2(tops[0] - top) / total
        cb = jnp.exp2(tops[1] - top) / total
        c_ref[h, 0:1, :] = ca
        c_ref[h, 1:2, :] = cb
        for k in range(nb):
            part = slice(k * rows, (k + 1) * rows)
            block = dqa_ref[h, :, part] * (ca[:, part] * scaling)
            block = block + dqb_ref[h, :, part] * (cb[:, part] * scaling)
            ref, spot = places[k]
            ref[spot * rows : (spot + 1) * rows, h * HD : (h + 1) * HD] = block.T.astype(ref.dtype)


def keyvalue_kernel(nz, nb, rows, scaling, *refs):
    qs, gs = refs[:nb], refs[nb : 2 * nb]
    c_ref, pa_ref, pb_ref, dsa_ref, dsb_ref = refs[2 * nb : 2 * nb + 5]
    outs = refs[2 * nb + 5 :]
    size = outs[0].shape[0]
    for i, (p_ref, ds_ref) in enumerate(((pa_ref, dsa_ref), (pb_ref, dsb_ref))):
        count = p_ref.shape[1] // size
        key_acc, value_acc = [None] * count, [None] * count
        for h in range(p_ref.shape[0]):
            lanes = slice(h * HD, (h + 1) * HD)
            c = c_ref[h, i : i + 1, :].astype(BF16)
            q = jnp.concatenate([m[:rows, lanes] for m in qs], axis=0)
            g = jnp.concatenate([m[:, lanes] for m in gs], axis=0)
            for z in range(count):
                part = slice(z * size, (z + 1) * size)
                key = dot(ds_ref[h, part, :] * c, q, 1, 0)
                value = dot(p_ref[h, part, :] * c, g, 1, 0)
                key_acc[z] = key if h == 0 else key_acc[z] + key
                value_acc[z] = value if h == 0 else value_acc[z] + value
        for z in range(count):
            out = outs[i * (nz // 2) + z]
            out[:, :HD] = (key_acc[z] * scaling).astype(out.dtype)
            out[:, HD:] = value_acc[z].astype(out.dtype)


def first_kernel(nz, dblk, rows, pair_ref, other_ref, near_ref, far_ref, dq_ref, own_ref, o_ref):
    own = (pair_ref[:rows, :].astype(F32) + other_ref[rows:, :].astype(F32)).astype(BF16)
    dq_ref[:rows, :] = own
    own_ref[...] = own
    dq_ref[rows:, :] = (pair_ref[rows:, :].astype(F32) + other_ref[:rows, :].astype(F32)).astype(BF16)
    dq = dq_ref[...]
    for k in range(nz):
        at = slice((2 * k + 1) * dblk, (2 * k + 2) * dblk)
        left = jnp.concatenate([near_ref[at, :], far_ref[at, :]], axis=1)
        o_ref[k * dblk : (k + 1) * dblk, :] = dot(left, dq, 1, 0).astype(BF16)


def second_kernel(nz, dblk, dq_ref, near_ref, far_ref, got_ref, *outs):
    dq = dq_ref[...]
    for k in range(nz):
        at = slice(2 * k * dblk, (2 * k + 1) * dblk)
        left = jnp.concatenate([near_ref[at, :], far_ref[at, :]], axis=1)
        total = dot(left, dq, 1, 0) + got_ref[k * dblk : (k + 1) * dblk, :].astype(F32)
        outs[k][...] = total.astype(outs[k].dtype)


def pair_kernel(*refs):
    n = len(refs) // 3
    for kept, got, out in zip(refs[:n], refs[n : 2 * n], refs[2 * n :]):
        out[...] = (kept[...] + got[...].astype(F32)).astype(BF16)


def zsum_kernel(nz, *refs):
    own_ref, rest_ref = refs[nz:]
    total = refs[0][...].astype(F32)
    for k in range(1, nz):
        total = total + refs[k][...].astype(F32)
    size = own_ref.shape[0]
    own_ref[...] = total[:size].astype(BF16)
    rest_ref[...] = total[size:].astype(BF16)


def dtarget_kernel(tp, idx_ref, x_ref, g_ref, *refs):
    dqs, w_ref = refs[:tp], refs[tp]
    mine, theirs = refs[tp + 1 : 2 * tp], refs[2 * tp : 3 * tp - 1]
    o_ref, acc = refs[3 * tp - 1 :]
    acc[...] = dot(dqs[0][...], w_ref[...], 1, 1)
    size = acc.shape[1] // 2
    for flip, halves in enumerate((mine, theirs)):
        at = pl.ds(pl.multiple_of((idx_ref[0] ^ flip) * size, size), size)
        for d in range(1, tp):
            acc[:, at] += dot(dqs[d][...], halves[d - 1][...], 1, 1)
    o_ref[...] = norm_back(x_ref[...], g_ref[...], acc[...]).astype(BF16)


def dsource_kernel(idx_ref, x_ref, g_ref, wk_ref, wv_ref, *refs):
    o_ref = refs[KVH]
    total = None
    for r in range(KVH):
        at = pl.ds(pl.multiple_of((idx_ref[0] ^ r) * HD, HD), HD)
        part = dot(refs[r][:, :HD], wk_ref[:, at], 1, 1) + dot(refs[r][:, HD:], wv_ref[:, at], 1, 1)
        total = part if total is None else total + part
    o_ref[...] = norm_back(x_ref[...], g_ref[...], total)


def whole(shape):
    return pl.BlockSpec(shape, lambda *_: (0,) * len(shape))


def estimate(flops, mib):
    return pl.CostEstimate(flops=flops, bytes_accessed=mib << 20, transcendentals=0)


def call(body, out_shape, args, flops=1 << 24, mib=2, mb=12, index=(), scratch=(), specs=None):
    outs = out_shape if isinstance(out_shape, list) else [out_shape]
    specs = specs or [whole(a.shape) for a in args]
    out_specs = [whole(o.shape) for o in outs]
    scalars = [i.astype(jnp.int32).reshape(1) for i in index]
    got = pl.pallas_call(
        body,
        grid_spec=pltpu.PrefetchScalarGridSpec(
            num_scalar_prefetch=len(scalars),
            grid=(1,),
            in_specs=specs,
            out_specs=out_specs,
            scratch_shapes=list(scratch),
        ),
        out_shape=outs,
        compiler_params=pltpu.CompilerParams(vmem_limit_bytes=mb << 20),
        cost_estimate=estimate(flops, mib),
    )(*scalars, *args)
    return got if isinstance(out_shape, list) else got[0]


def local(target, source, target_gain, source_gain, w_query, w_key, w_value, attended, d_attended):
    sp, tp = lax.axis_size("sp"), lax.axis_size("tp")
    me, mt = lax.axis_index("sp"), lax.axis_index("tp")
    rows, dim = target.shape
    srows = source.shape[0]
    width = w_query.shape[1]
    heads = width // HD
    group = tp // KVH
    nb = 4
    nz = sp // nb
    half = nb // 2
    scaling = HD ** (-0.5)
    kv_index = mt // group
    dblk = dim // sp
    steps = 4
    kvw = KVH * HD
    shape = jax.ShapeDtypeStruct
    t_gain, s_gain = target_gain.reshape(1, dim), source_gain.reshape(1, dim)

    hbm = pl.BlockSpec(memory_space=pltpu.HBM)
    near_rows = dim // 2
    by_head = call(
        functools.partial(source_kernel, steps),
        [shape((srows, 2 * HD), BF16)] * KVH,
        (source, s_gain, w_key, w_value),
        flops=4 * srows * dim * kvw,
        mb=FRONT_MIB,
        index=(kv_index,),
        specs=[hbm] * 4,
        scratch=[
            pltpu.VMEM((srows, dim), BF16),
            pltpu.VMEM((1, dim), F32),
            pltpu.VMEM((dim, kvw), BF16),
            pltpu.VMEM((dim, kvw), BF16),
            pltpu.VMEM((srows, kvw), BF16),
            pltpu.VMEM((srows, kvw), BF16),
            pltpu.SemaphoreType.DMA((2,)),
            pltpu.SemaphoreType.DMA((steps,)),
            pltpu.SemaphoreType.DMA((steps,)),
        ],
    )
    q_ext, near, far = call(
        functools.partial(target_kernel, steps, sp, half),
        [shape((rows + 16, width), BF16)] + [shape((near_rows, rows), BF16)] * 2,
        (target, t_gain, w_query, attended, d_attended),
        flops=2 * rows * dim * width,
        mb=FRONT_MIB,
        index=(me,),
        specs=[hbm] * 5,
        scratch=[
            pltpu.VMEM((rows, dim), BF16),
            pltpu.VMEM((1, dim), F32),
            pltpu.VMEM((dim, width), BF16),
            pltpu.VMEM((rows, width), BF16),
            pltpu.VMEM((rows, width), BF16),
            pltpu.VMEM((dim, rows), BF16),
            pltpu.SemaphoreType.DMA((4,)),
            pltpu.SemaphoreType.DMA((steps,)),
        ],
    )

    def away(x, k, step=None):
        return swap(x, "sp", (step or k) * nb)

    def gathered(blocks):
        odd = [away(blocks[k], k, 1) for k in range(1, nz, 2)]
        pairs = call(
            pair_kernel, [shape(x.shape, BF16) for x in odd[1:]], (*blocks[2::2], *odd[1:]), mib=1
        )
        return [blocks[0], odd[0]] + [away(x, 2 * i + 2) for i, x in enumerate(pairs)]

    rest = [swap(by_head[d // group], "tp", d) for d in range(1, tp)]
    kv_own = jnp.concatenate([by_head[0]] + rest, axis=0)
    chunks = [range(nz // 2), range(nz // 2, nz)]
    kvs = []
    for ks in chunks:
        kvs.append([kv_own if k == 0 else away(kv_own, k) for k in ks])
    qs = [q_ext] + [swap(q_ext, "sp", k) for k in range(1, nb)]
    gs = [d_attended] + [swap(d_attended, "sp", k) for k in range(1, nb)]
    far = swap(far, "sp", half)

    held, _ = lax.optimization_barrier((w_query, kv_own))
    piece = lax.dynamic_slice_in_dim(held, (me & 1) * (dim // 2), dim // 2, 0)
    wq_mine = [swap(piece, "tp", d) for d in range(1, tp)]
    wq_theirs = [swap(w, "sp", 1) for w in wq_mine]

    trows = nb * rows
    stshape = shape((heads, 8, trows), F32)
    dqshape = shape((heads, HD, trows), F32)

    def scores(c):
        part = sum(kv.shape[0] for kv in kvs[c])
        return call(
            functools.partial(scores_kernel, len(kvs[c]), nb, rows, scaling),
            [
                shape((heads, part, trows), BF16),
                stshape,
                shape((part, HD), BF16),
                shape((part, HD), BF16),
                shape((HD, part), BF16),
            ],
            (*kvs[c], *qs),
            flops=4 * heads * part * trows * HD,
        )

    def grads(probs, values, keys_t):
        return call(
            functools.partial(grads_kernel, nb, rows),
            [shape(probs.shape, BF16), dqshape],
            (values, keys_t, probs, *qs, *gs),
            flops=6 * probs.size * HD,
        )

    p_a, st_a, _, v_a, kt_a = scores(0)
    ds_a, dq_a = grads(p_a, v_a, kt_a)
    p_b, st_b, _, v_b, kt_b = scores(1)
    stats = call(functools.partial(lse_kernel, heads), shape((8 * -(-heads // 4), trows), F32), (st_a, st_b), mib=1)
    sts = [swap(stats, "sp", k) for k in range(1, nb)]
    ds_b, dq_b = grads(p_b, v_b, kt_b)
    coef, sent, kept = call(
        functools.partial(scale_kernel, nb, rows, heads, scaling),
        [stshape, shape((2 * rows, width), BF16), shape((2 * rows, width), F32)],
        (st_a, st_b, *sts, dq_a, dq_b),
    )
    src = tp * srows
    dkvs = call(
        functools.partial(keyvalue_kernel, nz, nb, rows, scaling),
        [shape((src, 2 * HD), BF16 if z % 2 else F32) for z in range(nz)],
        (*qs, *gs, coef, p_a, p_b, ds_a, ds_b),
        flops=6 * heads * nz * src * trows * HD,
    )

    pair_b = (kept + swap(sent, "sp", 1).astype(F32)).astype(BF16)
    other = swap(pair_b, "sp", half)

    dq_two, dq_own, partial = call(
        functools.partial(first_kernel, nz, dblk, rows),
        [shape((2 * rows, width), BF16), shape((rows, width), BF16), shape((nz * dblk, width), BF16)],
        (pair_b, other, near, far),
        flops=4 * rows * nz * dblk * width,
    )
    got = swap(partial, "sp", 1)
    mine = call(
        functools.partial(second_kernel, nz, dblk),
        [shape((dblk, width), BF16 if k % 2 else F32) for k in range(nz)],
        (dq_two, near, far, got),
        flops=4 * rows * nz * dblk * width,
    )
    d_w_query, *arrived = gathered(mine)
    for x in arrived:
        d_w_query = d_w_query + x.astype(F32)

    dqs = [dq_own] + [swap(dq_own, "tp", d) for d in range(1, tp)]
    d_target = call(
        functools.partial(dtarget_kernel, tp),
        shape((rows, dim), BF16),
        (target, t_gain, *dqs, w_query, *wq_mine, *wq_theirs),
        flops=2 * rows * dim * width * tp,
        index=(me & 1,),
        scratch=[pltpu.VMEM((rows, dim), F32)],
    )

    dkvs = gathered(dkvs)
    own, others = call(
        functools.partial(zsum_kernel, len(dkvs)),
        [shape((srows, 2 * HD), BF16), shape((src - srows, 2 * HD), BF16)],
        dkvs,
    )
    relative = [own] + [None] * (KVH - 1)
    for d in range(1, tp):
        block = swap(others[(d - 1) * srows : d * srows], "tp", d)
        r = d // group
        if relative[r] is None:
            relative[r] = block
        else:
            relative[r] = relative[r].astype(F32) + block.astype(F32)
    d_source = call(
        dsource_kernel,
        shape((srows, dim), F32),
        (source, s_gain, w_key, w_value, *[x.astype(BF16) for x in relative]),
        flops=4 * srows * dim * kvw,
        index=(kv_index,),
    )
    return (d_target, d_source, d_w_query)


def solution(mesh):
    return jax.shard_map(
        local,
        mesh=mesh,
        in_specs=(
            P("sp", None),
            P(("sp", "tp"), None),
            P(),
            P(),
            P(None, "tp"),
            P(),
            P(),
            P("sp", "tp"),
            P("sp", "tp"),
        ),
        out_specs=(P("sp", None), P(("sp", "tp"), None), P("sp", "tp")),
        check_vma=False,
    )
```

```python
import functools

import jax
import jax.numpy as jnp
from jax import lax
from jax.experimental import pallas as pl
from jax.experimental.pallas import tpu as pltpu
from jax.sharding import PartitionSpec as P


KVH = 2
HD = 128
EPS = 1e-06
LOG2E = 1.4426950408889634
FRONT_MIB = 60


F32 = jnp.float32
BF16 = jnp.bfloat16


def swap(x, axis, k):
    n = lax.axis_size(axis)
    return lax.ppermute(x, axis, [(i, i ^ k) for i in range(n)])


def dot(a, b, ca, cb):
    return lax.dot_general(a, b, (((ca,), (cb,)), ((), ())), preferred_element_type=F32)


def normed(x, gain):
    wide = x.astype(F32)
    inverse = lax.rsqrt(jnp.mean(wide * wide, axis=-1, keepdims=True) + EPS)
    return (wide * inverse * gain).astype(BF16)


def norm_back(x, gain, cotangent):
    wide = x.astype(F32)
    inverse = lax.rsqrt(jnp.mean(wide * wide, axis=-1, keepdims=True) + EPS)
    scaled = cotangent * gain
    inner = jnp.mean(wide * scaled, axis=-1, keepdims=True)
    return inverse * scaled - wide * (inverse * inverse * inverse * inner)


def chunk_copy(src, dst, sem, s, size):
    at = pl.ds(s * size, size)
    return pltpu.make_async_copy(src.at[at, :], dst.at[at, :], sem.at[s])


def source_kernel(steps, kv_ref, x_any, g_any, wk_any, wv_any, *refs):
    outs = refs[:KVH]
    x_ref, g_ref, wk_ref, wv_ref, k_ref, v_ref, sem, k_sem, v_sem = refs[KVH:]
    chunk = wk_ref.shape[0] // steps
    first = [
        pltpu.make_async_copy(x_any, x_ref, sem.at[0]),
        pltpu.make_async_copy(g_any, g_ref, sem.at[1]),
    ]
    wks = [chunk_copy(wk_any, wk_ref, k_sem, s, chunk) for s in range(steps)]
    wvs = [chunk_copy(wv_any, wv_ref, v_sem, s, chunk) for s in range(steps)]
    for copy in first:
        copy.start()
    for s in range(steps):
        wks[s].start()
        wvs[s].start()
    for copy in first:
        copy.wait()
    x_ref[...] = normed(x_ref[...], g_ref[...])
    k_acc, v_acc = None, None
    for s in range(steps):
        part = slice(s * chunk, (s + 1) * chunk)
        wks[s].wait()
        k = dot(x_ref[:, part], wk_ref[part, :], 1, 0)
        wvs[s].wait()
        v = dot(x_ref[:, part], wv_ref[part, :], 1, 0)
        k_acc = k if k_acc is None else k_acc + k
        v_acc = v if v_acc is None else v_acc + v
    k_ref[...] = k_acc.astype(BF16)
    v_ref[...] = v_acc.astype(BF16)
    for r in range(KVH):
        at = pl.ds(pl.multiple_of((kv_ref[0] ^ r) * HD, HD), HD)
        outs[r][:, :HD] = k_ref[:, at]
        outs[r][:, HD:] = v_ref[:, at]


def target_kernel(steps, sp, half, me_ref, x_any, g_any, wq_any, at_any, da_any, *refs):
    q_ref, near_ref, far_ref = refs[:3]
    x_ref, g_ref, wq_ref, at_ref, da_ref, nt_ref, sem, q_sem = refs[3:]
    dim = wq_ref.shape[0]
    chunk = dim // steps
    rows = x_ref.shape[0]
    dblk = dim // sp
    pairs = ((x_any, x_ref), (g_any, g_ref), (da_any, da_ref), (at_any, at_ref))
    copies = [pltpu.make_async_copy(a, b, sem.at[i]) for i, (a, b) in enumerate(pairs)]
    wqs = [chunk_copy(wq_any, wq_ref, q_sem, s, chunk) for s in range(steps)]
    for copy in copies + wqs:
        copy.start()
    for copy in copies[:2]:
        copy.wait()
    x_ref[...] = normed(x_ref[...], g_ref[...])
    for s in range(steps):
        part = slice(s * chunk, (s + 1) * chunk)
        nt_ref[part, :] = x_ref[:, part].T
    for copy in copies[2:]:
        copy.wait()
    prod = da_ref[...].astype(F32) * at_ref[...].astype(F32)
    q_ref[rows:, :] = jnp.zeros_like(q_ref[rows:, :])
    for h in range(prod.shape[1] // HD):
        d = jnp.sum(prod[:, h * HD : (h + 1) * HD].T, axis=0, keepdims=True)
        q_ref[rows : rows + 1, h * HD : h * HD + rows] = d.astype(BF16)
    me = me_ref[0]
    n = 0
    for j in range(sp):
        if j & half:
            continue
        here = pl.multiple_of((me ^ j) * dblk, dblk)
        there = pl.multiple_of((me ^ j ^ half) * dblk, dblk)
        near_ref[n * dblk : (n + 1) * dblk, :] = nt_ref[pl.ds(here, dblk), :]
        far_ref[n * dblk : (n + 1) * dblk, :] = nt_ref[pl.ds(there, dblk), :]
        n += 1
    q_acc = None
    for s in range(steps):
        part = slice(s * chunk, (s + 1) * chunk)
        wqs[s].wait()
        q = dot(x_ref[:, part], wq_ref[part, :], 1, 0)
        q_acc = q if q_acc is None else q_acc + q
    q_ref[:rows, :] = q_acc.astype(BF16)


def scores_kernel(nk, nb, rows, scaling, *refs):
    kvs, qs = refs[:nk], refs[nk : nk + nb]
    p_ref, st_ref, k_ref, v_ref, kt_ref = refs[nk + nb :]
    at = 0
    for kv in kvs:
        size = kv.shape[0]
        k_ref[at : at + size, :] = kv[:, :HD]
        v_ref[at : at + size, :] = kv[:, HD:]
        at += size
    kt_ref[...] = k_ref[...].T
    for h in range(p_ref.shape[0]):
        lanes = slice(h * HD, (h + 1) * HD)
        for pair in range(nb // 2):
            q = jnp.concatenate(
                [qs[2 * pair + i][:rows, lanes] for i in range(2)], axis=0
            )
            cols = slice(pair * 2 * rows, (pair + 1) * 2 * rows)
            s = dot(k_ref[...], q, 1, 1)
            top = jnp.max(s, axis=0, keepdims=True)
            p = jnp.exp2((s - top) * (scaling * LOG2E))
            p_ref[h, :, cols] = p.astype(BF16)
            st_ref[h, 0:1, cols] = top * (scaling * LOG2E)
            st_ref[h, 1:2, cols] = jnp.sum(p, axis=0, keepdims=True)


def grads_kernel(nb, rows, v_ref, kt_ref, p_ref, *refs):
    qs, gs = refs[:nb], refs[nb : 2 * nb]
    ds_ref, dq_ref = refs[2 * nb :]
    items = [(h, pair) for h in range(p_ref.shape[0]) for pair in range(nb // 2)]

    def d_weights(h, pair):
        lanes = slice(h * HD, (h + 1) * HD)
        g = jnp.concatenate([gs[2 * pair + i][:, lanes] for i in range(2)], axis=0)
        return dot(v_ref[...], g, 1, 1)

    ahead = d_weights(*items[0])
    for n, (h, pair) in enumerate(items):
        lanes = slice(h * HD, (h + 1) * HD)
        cols = slice(pair * 2 * rows, (pair + 1) * 2 * rows)
        delta = jnp.concatenate(
            [qs[2 * pair + i][rows : rows + 1, lanes] for i in range(2)], axis=1
        ).astype(F32)
        ds = (p_ref[h, :, cols].astype(F32) * (ahead - delta)).astype(BF16)
        ds_ref[h, :, cols] = ds
        if n + 1 < len(items):
            ahead = d_weights(*items[n + 1])
        dq_ref[h, :, cols] = dot(kt_ref[...], ds, 1, 0)


def lse_kernel(heads, *refs):
    o_ref = refs[-1]
    o_ref[...] = jnp.zeros_like(o_ref)
    for h in range(heads):
        tops = [r[h, 0:1, :] for r in refs[:-1]]
        top = functools.reduce(jnp.maximum, tops)
        total = sum(r[h, 1:2, :] * jnp.exp2(t - top) for r, t in zip(refs[:-1], tops))
        o_ref[h : h + 1, :] = top
        o_ref[heads + h : heads + h + 1, :] = total


def scale_kernel(nc, nb, rows, heads, scaling, *refs):
    owns, sts, dqs = refs[:nc], refs[nc : nc + nb - 1], refs[nc + nb - 1 : 2 * nc + nb - 1]
    c_ref, sent_ref, kept_ref = refs[2 * nc + nb - 1 :]
    places = [(kept_ref, 0), (sent_ref, 0), (kept_ref, 1), (sent_ref, 1)]
    for h in range(heads):
        tops = [r[h, 0:1, :] for r in owns]
        sums = [r[h, 1:2, :] for r in owns]
        for k in range(1, nb):
            order = [slice((j ^ k) * rows, (j ^ k) * rows + rows) for j in range(nb)]
            st, low = sts[k - 1], heads + h
            tops.append(jnp.concatenate([st[h : h + 1, o] for o in order], axis=1))
            sums.append(jnp.concatenate([st[low : low + 1, o] for o in order], axis=1))
        top = functools.reduce(jnp.maximum, tops)
        total = sum(s * jnp.exp2(t - top) for t, s in zip(tops, sums))
        cs = [jnp.exp2(t - top) / total for t in tops[:nc]]
        for i, c in enumerate(cs):
            c_ref[h, i : i + 1, :] = c
        for k in range(nb):
            part = slice(k * rows, (k + 1) * rows)
            block = sum(r[h, :, part] * (c[:, part] * scaling) for r, c in zip(dqs, cs))
            ref, spot = places[k]
            ref[spot * rows : (spot + 1) * rows, h * HD : (h + 1) * HD] = block.T.astype(ref.dtype)


def keyvalue_kernel(places, nc, nb, rows, scaling, *refs):
    qs, gs, c_ref = refs[:nb], refs[nb : 2 * nb], refs[2 * nb]
    ps, dss = refs[2 * nb + 1 : 2 * nb + 1 + nc], refs[2 * nb + 1 + nc : 2 * nb + 1 + 2 * nc]
    outs = refs[2 * nb + 1 + 2 * nc :]
    size = outs[0].shape[0]
    count = len(places)
    key_acc, value_acc = [None] * count, [None] * count
    for h in range(ps[0].shape[0]):
        lanes = slice(h * HD, (h + 1) * HD)
        q = jnp.concatenate([m[:rows, lanes] for m in qs], axis=0)
        g = jnp.concatenate([m[:, lanes] for m in gs], axis=0)
        for i, (chunk, spot) in enumerate(places):
            c = c_ref[h, chunk : chunk + 1, :].astype(BF16)
            part = slice(spot * size, (spot + 1) * size)
            key = dot(dss[chunk][h, part, :] * c, q, 1, 0)
            value = dot(ps[chunk][h, part, :] * c, g, 1, 0)
            key_acc[i] = key if h == 0 else key_acc[i] + key
            value_acc[i] = value if h == 0 else value_acc[i] + value
    for i, out in enumerate(outs):
        out[:, :HD] = (key_acc[i] * scaling).astype(out.dtype)
        out[:, HD:] = value_acc[i].astype(out.dtype)


def first_kernel(nz, dblk, rows, pair_ref, other_ref, near_ref, far_ref, dq_ref, own_ref, o_ref):
    own = (pair_ref[:rows, :].astype(F32) + other_ref[rows:, :].astype(F32)).astype(BF16)
    dq_ref[:rows, :] = own
    own_ref[...] = own
    dq_ref[rows:, :] = (pair_ref[rows:, :].astype(F32) + other_ref[:rows, :].astype(F32)).astype(BF16)
    dq = dq_ref[...]
    for k in range(nz):
        at = slice((2 * k + 1) * dblk, (2 * k + 2) * dblk)
        left = jnp.concatenate([near_ref[at, :], far_ref[at, :]], axis=1)
        o_ref[k * dblk : (k + 1) * dblk, :] = dot(left, dq, 1, 0).astype(BF16)


def second_kernel(nz, dblk, dq_ref, near_ref, far_ref, got_ref, *outs):
    dq = dq_ref[...]
    for k in range(nz):
        at = slice(2 * k * dblk, (2 * k + 1) * dblk)
        left = jnp.concatenate([near_ref[at, :], far_ref[at, :]], axis=1)
        total = dot(left, dq, 1, 0) + got_ref[k * dblk : (k + 1) * dblk, :].astype(F32)
        outs[k][...] = total.astype(outs[k].dtype)


def pair_kernel(*refs):
    n = len(refs) // 3
    for kept, got, out in zip(refs[:n], refs[n : 2 * n], refs[2 * n :]):
        out[...] = (kept[...] + got[...].astype(F32)).astype(BF16)


def zsum_kernel(nz, *refs):
    own_ref, rest_ref = refs[nz:]
    total = refs[0][...].astype(F32)
    for k in range(1, nz):
        total = total + refs[k][...].astype(F32)
    size = own_ref.shape[0]
    own_ref[...] = total[:size].astype(BF16)
    rest_ref[...] = total[size:].astype(BF16)


def dtarget_kernel(tp, idx_ref, x_ref, g_ref, *refs):
    dqs, w_ref = refs[:tp], refs[tp]
    mine, theirs = refs[tp + 1 : 2 * tp], refs[2 * tp : 3 * tp - 1]
    o_ref, acc = refs[3 * tp - 1 :]
    acc[...] = dot(dqs[0][...], w_ref[...], 1, 1)
    size = acc.shape[1] // 2
    for flip, halves in enumerate((mine, theirs)):
        at = pl.ds(pl.multiple_of((idx_ref[0] ^ flip) * size, size), size)
        for d in range(1, tp):
            acc[:, at] += dot(dqs[d][...], halves[d - 1][...], 1, 1)
    o_ref[...] = norm_back(x_ref[...], g_ref[...], acc[...]).astype(BF16)


def dsource_kernel(idx_ref, x_ref, g_ref, wk_ref, wv_ref, *refs):
    o_ref = refs[KVH]
    total = None
    for r in range(KVH):
        at = pl.ds(pl.multiple_of((idx_ref[0] ^ r) * HD, HD), HD)
        part = dot(refs[r][:, :HD], wk_ref[:, at], 1, 1) + dot(refs[r][:, HD:], wv_ref[:, at], 1, 1)
        total = part if total is None else total + part
    o_ref[...] = norm_back(x_ref[...], g_ref[...], total)


def whole(shape):
    return pl.BlockSpec(shape, lambda *_: (0,) * len(shape))


def estimate(flops, mib):
    return pl.CostEstimate(flops=flops, bytes_accessed=mib << 20, transcendentals=0)


def call(body, out_shape, args, flops=1 << 24, mib=2, mb=12, index=(), scratch=(), specs=None):
    outs = out_shape if isinstance(out_shape, list) else [out_shape]
    specs = specs or [whole(a.shape) for a in args]
    out_specs = [whole(o.shape) for o in outs]
    scalars = [i.astype(jnp.int32).reshape(1) for i in index]
    got = pl.pallas_call(
        body,
        grid_spec=pltpu.PrefetchScalarGridSpec(
            num_scalar_prefetch=len(scalars),
            grid=(1,),
            in_specs=specs,
            out_specs=out_specs,
            scratch_shapes=list(scratch),
        ),
        out_shape=outs,
        compiler_params=pltpu.CompilerParams(vmem_limit_bytes=mb << 20),
        cost_estimate=estimate(flops, mib),
    )(*scalars, *args)
    return got if isinstance(out_shape, list) else got[0]


def local(target, source, target_gain, source_gain, w_query, w_key, w_value, attended, d_attended):
    sp, tp = lax.axis_size("sp"), lax.axis_size("tp")
    me, mt = lax.axis_index("sp"), lax.axis_index("tp")
    rows, dim = target.shape
    srows = source.shape[0]
    width = w_query.shape[1]
    heads = width // HD
    group = tp // KVH
    nb = 4
    nz = sp // nb
    half = nb // 2
    scaling = HD ** (-0.5)
    kv_index = mt // group
    dblk = dim // sp
    steps = 4
    kvw = KVH * HD
    shape = jax.ShapeDtypeStruct
    t_gain, s_gain = target_gain.reshape(1, dim), source_gain.reshape(1, dim)

    hbm = pl.BlockSpec(memory_space=pltpu.HBM)
    near_rows = dim // 2
    by_head = call(
        functools.partial(source_kernel, steps),
        [shape((srows, 2 * HD), BF16)] * KVH,
        (source, s_gain, w_key, w_value),
        flops=4 * srows * dim * kvw,
        mb=FRONT_MIB,
        index=(kv_index,),
        specs=[hbm] * 4,
        scratch=[
            pltpu.VMEM((srows, dim), BF16),
            pltpu.VMEM((1, dim), F32),
            pltpu.VMEM((dim, kvw), BF16),
            pltpu.VMEM((dim, kvw), BF16),
            pltpu.VMEM((srows, kvw), BF16),
            pltpu.VMEM((srows, kvw), BF16),
            pltpu.SemaphoreType.DMA((2,)),
            pltpu.SemaphoreType.DMA((steps,)),
            pltpu.SemaphoreType.DMA((steps,)),
        ],
    )
    q_ext, near, far = call(
        functools.partial(target_kernel, steps, sp, half),
        [shape((rows + 16, width), BF16)] + [shape((near_rows, rows), BF16)] * 2,
        (target, t_gain, w_query, attended, d_attended),
        flops=2 * rows * dim * width,
        mb=FRONT_MIB,
        index=(me,),
        specs=[hbm] * 5,
        scratch=[
            pltpu.VMEM((rows, dim), BF16),
            pltpu.VMEM((1, dim), F32),
            pltpu.VMEM((dim, width), BF16),
            pltpu.VMEM((rows, width), BF16),
            pltpu.VMEM((rows, width), BF16),
            pltpu.VMEM((dim, rows), BF16),
            pltpu.SemaphoreType.DMA((4,)),
            pltpu.SemaphoreType.DMA((steps,)),
        ],
    )

    def away(x, k, step=None):
        return swap(x, "sp", (step or k) * nb)

    def gathered(blocks):
        odd = [away(blocks[k], k, 1) for k in range(1, nz, 2)]
        pairs = call(
            pair_kernel, [shape(x.shape, BF16) for x in odd[1:]], (*blocks[2::2], *odd[1:]), mib=1
        )
        return [blocks[0], odd[0]] + [away(x, 2 * i + 2) for i, x in enumerate(pairs)]

    rest = [swap(by_head[d // group], "tp", d) for d in range(1, tp)]
    kv_own = jnp.concatenate([by_head[0]] + rest, axis=0)
    late = list(range(nz // 2 + 1, nz, 2))
    chunks = [[k for k in range(nz) if k not in late], late]
    chunk_of = {k: c for c, ks in enumerate(chunks) for k in ks}
    at_hand = {0: kv_own}
    for k in list(range(2, nz, 2)) + list(range(1, nz, 2)):
        at_hand[k] = away(at_hand[k - 1] if k % 2 else kv_own, k, 1 if k % 2 else k)
    kvs = [[at_hand[k] for k in ks] for ks in chunks]

    qs = [q_ext] + [swap(q_ext, "sp", k) for k in range(1, nb)]
    gs = [d_attended] + [swap(d_attended, "sp", k) for k in range(1, nb)]
    far = swap(far, "sp", half)

    held, _ = lax.optimization_barrier((w_query, kv_own))
    piece = lax.dynamic_slice_in_dim(held, (me & 1) * (dim // 2), dim // 2, 0)
    wq_mine = [swap(piece, "tp", d) for d in range(1, tp)]
    wq_theirs = [swap(w, "sp", 1) for w in wq_mine]

    trows = nb * rows
    stshape = shape((heads, 8, trows), F32)
    dqshape = shape((heads, HD, trows), F32)

    def scores(c):
        part = sum(kv.shape[0] for kv in kvs[c])
        return call(
            functools.partial(scores_kernel, len(kvs[c]), nb, rows, scaling),
            [
                shape((heads, part, trows), BF16),
                stshape,
                shape((part, HD), BF16),
                shape((part, HD), BF16),
                shape((HD, part), BF16),
            ],
            (*kvs[c], *qs),
            flops=4 * heads * part * trows * HD,
        )

    def grads(probs, values, keys_t):
        return call(
            functools.partial(grads_kernel, nb, rows),
            [shape(probs.shape, BF16), dqshape],
            (values, keys_t, probs, *qs, *gs),
            flops=6 * probs.size * HD,
        )

    nc = len(chunks)
    probs, own_stats, _, values, keys_t = zip(*[scores(c) for c in range(nc)])
    stats = call(
        functools.partial(lse_kernel, heads),
        shape((8 * -(-heads // 4), trows), F32),
        own_stats,
        mib=1,
    )
    sts = [swap(stats, "sp", k) for k in range(1, nb)]
    d_scores, dq_parts = zip(*[grads(probs[c], values[c], keys_t[c]) for c in range(nc)])
    coef, sent, kept = call(
        functools.partial(scale_kernel, nc, nb, rows, heads, scaling),
        [stshape, shape((2 * rows, width), BF16), shape((2 * rows, width), F32)],
        (*own_stats, *sts, *dq_parts),
    )
    src = tp * srows
    dkvs = [None] * nz
    for ks in (range(1, nz, 2), range(0, nz, 2)):
        places = [(chunk_of[k], chunks[chunk_of[k]].index(k)) for k in ks]
        results = call(
            functools.partial(keyvalue_kernel, places, nc, nb, rows, scaling),
            [shape((src, 2 * HD), BF16 if k % 2 else F32) for k in ks],
            (*qs, *gs, coef, *probs, *d_scores),
            flops=3 * heads * nz * src * trows * HD,
        )
        for k, x in zip(ks, results):
            dkvs[k] = x

    pair_b = (kept + swap(sent, "sp", 1).astype(F32)).astype(BF16)
    other = swap(pair_b, "sp", half)

    dq_two, dq_own, partial = call(
        functools.partial(first_kernel, nz, dblk, rows),
        [shape((2 * rows, width), BF16), shape((rows, width), BF16), shape((nz * dblk, width), BF16)],
        (pair_b, other, near, far),
        flops=4 * rows * nz * dblk * width,
    )
    got = swap(partial, "sp", 1)
    mine = call(
        functools.partial(second_kernel, nz, dblk),
        [shape((dblk, width), BF16 if k % 2 else F32) for k in range(nz)],
        (dq_two, near, far, got),
        flops=4 * rows * nz * dblk * width,
    )
    d_w_query, *arrived = gathered(mine)
    for x in arrived:
        d_w_query = d_w_query + x.astype(F32)

    dqs = [dq_own] + [swap(dq_own, "tp", d) for d in range(1, tp)]
    d_target = call(
        functools.partial(dtarget_kernel, tp),
        shape((rows, dim), BF16),
        (target, t_gain, *dqs, w_query, *wq_mine, *wq_theirs),
        flops=2 * rows * dim * width * tp,
        index=(me & 1,),
        scratch=[pltpu.VMEM((rows, dim), F32)],
    )

    dkvs = gathered(dkvs)
    own, others = call(
        functools.partial(zsum_kernel, len(dkvs)),
        [shape((srows, 2 * HD), BF16), shape((src - srows, 2 * HD), BF16)],
        dkvs,
    )
    relative = [own] + [None] * (KVH - 1)
    for d in range(1, tp):
        block = swap(others[(d - 1) * srows : d * srows], "tp", d)
        r = d // group
        if relative[r] is None:
            relative[r] = block
        else:
            relative[r] = relative[r].astype(F32) + block.astype(F32)
    d_source = call(
        dsource_kernel,
        shape((srows, dim), F32),
        (source, s_gain, w_key, w_value, *[x.astype(BF16) for x in relative]),
        flops=4 * srows * dim * kvw,
        index=(kv_index,),
    )
    return (d_target, d_source, d_w_query)


def solution(mesh):
    return jax.shard_map(
        local,
        mesh=mesh,
        in_specs=(
            P("sp", None),
            P(("sp", "tp"), None),
            P(),
            P(),
            P(None, "tp"),
            P(),
            P(),
            P("sp", "tp"),
            P("sp", "tp"),
        ),
        out_specs=(P("sp", None), P(("sp", "tp"), None), P("sp", "tp")),
        check_vma=False,
    )
```

```python
import functools

import jax
import jax.numpy as jnp
from jax import lax
from jax.experimental import pallas as pl
from jax.experimental.pallas import tpu as pltpu
from jax.sharding import PartitionSpec as P


KVH = 2
HD = 128
EPS = 1e-06
LOG2E = 1.4426950408889634
FRONT_MIB = 16


F32 = jnp.float32
BF16 = jnp.bfloat16


def swap(x, axis, k):
    n = lax.axis_size(axis)
    return lax.ppermute(x, axis, [(i, i ^ k) for i in range(n)])


def dot(a, b, ca, cb):
    return lax.dot_general(a, b, (((ca,), (cb,)), ((), ())), preferred_element_type=F32)


def normed(x, gain):
    wide = x.astype(F32)
    inverse = lax.rsqrt(jnp.mean(wide * wide, axis=-1, keepdims=True) + EPS)
    return (wide * inverse * gain).astype(BF16)


def norm_back(x, gain, cotangent):
    wide = x.astype(F32)
    inverse = lax.rsqrt(jnp.mean(wide * wide, axis=-1, keepdims=True) + EPS)
    scaled = cotangent * gain
    inner = jnp.mean(wide * scaled, axis=-1, keepdims=True)
    return inverse * scaled - wide * (inverse * inverse * inverse * inner)


def chunk_copy(src, dst, sem, s, size):
    at = pl.ds(s * size, size)
    return pltpu.make_async_copy(src.at[at, :], dst.at[at, :], sem.at[s])


def source_kernel(steps, kv_ref, x_any, g_any, wk_any, wv_any, *refs):
    outs = refs[:KVH]
    x_ref, g_ref, wk_ref, wv_ref, k_ref, v_ref, sem, k_sem, v_sem = refs[KVH:]
    chunk = wk_ref.shape[0] // steps
    first = [
        pltpu.make_async_copy(x_any, x_ref, sem.at[0]),
        pltpu.make_async_copy(g_any, g_ref, sem.at[1]),
    ]
    wks = [chunk_copy(wk_any, wk_ref, k_sem, s, chunk) for s in range(steps)]
    wvs = [chunk_copy(wv_any, wv_ref, v_sem, s, chunk) for s in range(steps)]
    for copy in first:
        copy.start()
    for s in range(steps):
        wks[s].start()
        wvs[s].start()
    for copy in first:
        copy.wait()
    x_ref[...] = normed(x_ref[...], g_ref[...])
    k_acc, v_acc = None, None
    for s in range(steps):
        part = slice(s * chunk, (s + 1) * chunk)
        wks[s].wait()
        k = dot(x_ref[:, part], wk_ref[part, :], 1, 0)
        wvs[s].wait()
        v = dot(x_ref[:, part], wv_ref[part, :], 1, 0)
        k_acc = k if k_acc is None else k_acc + k
        v_acc = v if v_acc is None else v_acc + v
    k_ref[...] = k_acc.astype(BF16)
    v_ref[...] = v_acc.astype(BF16)
    for r in range(KVH):
        at = pl.ds(pl.multiple_of((kv_ref[0] ^ r) * HD, HD), HD)
        outs[r][:, :HD] = k_ref[:, at]
        outs[r][:, HD:] = v_ref[:, at]


def target_kernel(steps, sp, half, me_ref, x_any, g_any, wq_any, at_any, da_any, *refs):
    q_ref, near_ref, far_ref = refs[:3]
    x_ref, g_ref, wq_ref, at_ref, da_ref, nt_ref, sem, q_sem = refs[3:]
    dim = wq_ref.shape[0]
    chunk = dim // steps
    rows = x_ref.shape[0]
    dblk = dim // sp
    pairs = ((x_any, x_ref), (g_any, g_ref), (da_any, da_ref), (at_any, at_ref))
    copies = [pltpu.make_async_copy(a, b, sem.at[i]) for i, (a, b) in enumerate(pairs)]
    wqs = [chunk_copy(wq_any, wq_ref, q_sem, s, chunk) for s in range(steps)]
    for copy in copies + wqs:
        copy.start()
    for copy in copies[:2]:
        copy.wait()
    x_ref[...] = normed(x_ref[...], g_ref[...])
    for s in range(steps):
        part = slice(s * chunk, (s + 1) * chunk)
        nt_ref[part, :] = x_ref[:, part].T
    for copy in copies[2:]:
        copy.wait()
    prod = da_ref[...].astype(F32) * at_ref[...].astype(F32)
    q_ref[rows:, :] = jnp.zeros_like(q_ref[rows:, :])
    for h in range(prod.shape[1] // HD):
        d = jnp.sum(prod[:, h * HD : (h + 1) * HD].T, axis=0, keepdims=True)
        q_ref[rows : rows + 1, h * HD : h * HD + rows] = d.astype(BF16)
    me = me_ref[0]
    n = 0
    for j in range(sp):
        if j & half:
            continue
        here = pl.multiple_of((me ^ j) * dblk, dblk)
        there = pl.multiple_of((me ^ j ^ half) * dblk, dblk)
        near_ref[n * dblk : (n + 1) * dblk, :] = nt_ref[pl.ds(here, dblk), :]
        far_ref[n * dblk : (n + 1) * dblk, :] = nt_ref[pl.ds(there, dblk), :]
        n += 1
    q_acc = None
    for s in range(steps):
        part = slice(s * chunk, (s + 1) * chunk)
        wqs[s].wait()
        q = dot(x_ref[:, part], wq_ref[part, :], 1, 0)
        q_acc = q if q_acc is None else q_acc + q
    q_ref[:rows, :] = q_acc.astype(BF16)


def cat_kernel(*refs):
    *parts, k_out, v_out = refs
    size = parts[0].shape[0]
    for i, r in enumerate(parts):
        k_out[i * size : (i + 1) * size, :] = r[:, :HD]
        v_out[i * size : (i + 1) * size, :] = r[:, HD:]


def stack(parts, out):
    size = parts[0].shape[0]
    for i, r in enumerate(parts):
        out[i * size : (i + 1) * size, :] = r[...]


def scores_kernel(nk, nb, rows, scaling, *refs):
    qs = refs[nk : nk + nb]
    p_ref, st_ref, kt_ref, k_ref = refs[nk + nb :]
    stack(refs[:nk], k_ref)
    kt_ref[...] = k_ref[...].T
    for h in range(p_ref.shape[0]):
        lanes = slice(h * HD, (h + 1) * HD)
        for pair in range(nb // 2):
            q = jnp.concatenate(
                [qs[2 * pair + i][:rows, lanes] for i in range(2)], axis=0
            )
            cols = slice(pair * 2 * rows, (pair + 1) * 2 * rows)
            s = dot(k_ref[...], q, 1, 1)
            top = jnp.max(s, axis=0, keepdims=True)
            p = jnp.exp2((s - top) * (scaling * LOG2E))
            p_ref[h, :, cols] = p.astype(BF16)
            st_ref[h, 0:1, cols] = top * (scaling * LOG2E)
            st_ref[h, 1:2, cols] = jnp.sum(p, axis=0, keepdims=True)


def grads_kernel(nk, nb, rows, *refs):
    kt_ref, p_ref = refs[nk : nk + 2]
    qs, gs = refs[nk + 2 : nk + 2 + nb], refs[nk + 2 + nb : nk + 2 + 2 * nb]
    ds_ref, dq_ref, v_ref = refs[nk + 2 + 2 * nb :]
    stack(refs[:nk], v_ref)
    items = [(h, pair) for h in range(p_ref.shape[0]) for pair in range(nb // 2)]

    def d_weights(h, pair):
        lanes = slice(h * HD, (h + 1) * HD)
        g = jnp.concatenate([gs[2 * pair + i][:, lanes] for i in range(2)], axis=0)
        return dot(v_ref[...], g, 1, 1)

    ahead = d_weights(*items[0])
    for n, (h, pair) in enumerate(items):
        lanes = slice(h * HD, (h + 1) * HD)
        cols = slice(pair * 2 * rows, (pair + 1) * 2 * rows)
        delta = jnp.concatenate(
            [qs[2 * pair + i][rows : rows + 1, lanes] for i in range(2)], axis=1
        ).astype(F32)
        ds = (p_ref[h, :, cols].astype(F32) * (ahead - delta)).astype(BF16)
        ds_ref[h, :, cols] = ds
        if n + 1 < len(items):
            ahead = d_weights(*items[n + 1])
        dq_ref[h, :, cols] = dot(kt_ref[...], ds, 1, 0)


def lse_kernel(heads, *refs):
    o_ref = refs[-1]
    o_ref[...] = jnp.zeros_like(o_ref)
    for h in range(heads):
        tops = [r[h, 0:1, :] for r in refs[:-1]]
        top = functools.reduce(jnp.maximum, tops)
        total = sum(r[h, 1:2, :] * jnp.exp2(t - top) for r, t in zip(refs[:-1], tops))
        o_ref[h : h + 1, :] = top
        o_ref[heads + h : heads + h + 1, :] = total


def scale_kernel(nc, nb, rows, heads, scaling, *refs):
    owns, sts, dqs = refs[:nc], refs[nc : nc + nb - 1], refs[nc + nb - 1 : 2 * nc + nb - 1]
    c_ref, sent_ref, kept_ref = refs[2 * nc + nb - 1 :]
    places = [(kept_ref, 0), (sent_ref, 0), (kept_ref, 1), (sent_ref, 1)]
    for h in range(heads):
        tops = [r[h, 0:1, :] for r in owns]
        sums = [r[h, 1:2, :] for r in owns]
        for k in range(1, nb):
            order = [slice((j ^ k) * rows, (j ^ k) * rows + rows) for j in range(nb)]
            st, low = sts[k - 1], heads + h
            tops.append(jnp.concatenate([st[h : h + 1, o] for o in order], axis=1))
            sums.append(jnp.concatenate([st[low : low + 1, o] for o in order], axis=1))
        top = functools.reduce(jnp.maximum, tops)
        total = sum(s * jnp.exp2(t - top) for t, s in zip(tops, sums))
        cs = [jnp.exp2(t - top) / total for t in tops[:nc]]
        for i, c in enumerate(cs):
            c_ref[h, i : i + 1, :] = c
        for k in range(nb):
            part = slice(k * rows, (k + 1) * rows)
            block = sum(r[h, :, part] * (c[:, part] * scaling) for r, c in zip(dqs, cs))
            ref, spot = places[k]
            ref[spot * rows : (spot + 1) * rows, h * HD : (h + 1) * HD] = block.T.astype(ref.dtype)


def keyvalue_kernel(places, nc, nb, rows, scaling, *refs):
    qs, gs, c_ref = refs[:nb], refs[nb : 2 * nb], refs[2 * nb]
    ps, dss = refs[2 * nb + 1 : 2 * nb + 1 + nc], refs[2 * nb + 1 + nc : 2 * nb + 1 + 2 * nc]
    outs = refs[2 * nb + 1 + 2 * nc :]
    size = outs[0].shape[0]
    count = len(places)
    key_acc, value_acc = [None] * count, [None] * count
    for h in range(ps[0].shape[0]):
        lanes = slice(h * HD, (h + 1) * HD)
        q = jnp.concatenate([m[:rows, lanes] for m in qs], axis=0)
        g = jnp.concatenate([m[:, lanes] for m in gs], axis=0)
        for i, (chunk, spot) in enumerate(places):
            c = c_ref[h, chunk : chunk + 1, :].astype(BF16)
            part = slice(spot * size, (spot + 1) * size)
            key = dot(dss[chunk][h, part, :] * c, q, 1, 0)
            value = dot(ps[chunk][h, part, :] * c, g, 1, 0)
            key_acc[i] = key if h == 0 else key_acc[i] + key
            value_acc[i] = value if h == 0 else value_acc[i] + value
    for i, out in enumerate(outs):
        out[:, :HD] = (key_acc[i] * scaling).astype(out.dtype)
        out[:, HD:] = value_acc[i].astype(out.dtype)


def first_kernel(nz, dblk, rows, pair_ref, other_ref, near_ref, far_ref, dq_ref, own_ref, o_ref):
    own = (pair_ref[:rows, :].astype(F32) + other_ref[rows:, :].astype(F32)).astype(BF16)
    dq_ref[:rows, :] = own
    own_ref[...] = own
    dq_ref[rows:, :] = (pair_ref[rows:, :].astype(F32) + other_ref[:rows, :].astype(F32)).astype(BF16)
    dq = dq_ref[...]
    for k in range(nz):
        at = slice((2 * k + 1) * dblk, (2 * k + 2) * dblk)
        left = jnp.concatenate([near_ref[at, :], far_ref[at, :]], axis=1)
        o_ref[k * dblk : (k + 1) * dblk, :] = dot(left, dq, 1, 0).astype(BF16)


def second_kernel(nz, dblk, dq_ref, near_ref, far_ref, got_ref, *outs):
    dq = dq_ref[...]
    for k in range(nz):
        at = slice(2 * k * dblk, (2 * k + 1) * dblk)
        left = jnp.concatenate([near_ref[at, :], far_ref[at, :]], axis=1)
        total = dot(left, dq, 1, 0) + got_ref[k * dblk : (k + 1) * dblk, :].astype(F32)
        outs[k][...] = total.astype(outs[k].dtype)


def pair_kernel(*refs):
    n = len(refs) // 3
    for kept, got, out in zip(refs[:n], refs[n : 2 * n], refs[2 * n :]):
        out[...] = (kept[...] + got[...].astype(F32)).astype(BF16)


def zsum_kernel(nz, *refs):
    own_ref, rest_ref = refs[nz:]
    total = refs[0][...].astype(F32)
    for k in range(1, nz):
        total = total + refs[k][...].astype(F32)
    size = own_ref.shape[0]
    own_ref[...] = total[:size].astype(BF16)
    rest_ref[...] = total[size:].astype(BF16)


def dtarget_kernel(tp, idx_ref, x_ref, g_ref, *refs):
    dqs, w_ref = refs[:tp], refs[tp]
    mine, theirs = refs[tp + 1 : 2 * tp], refs[2 * tp : 3 * tp - 1]
    o_ref, acc = refs[3 * tp - 1 :]
    acc[...] = dot(dqs[0][...], w_ref[...], 1, 1)
    size = acc.shape[1] // 2
    for flip, halves in enumerate((mine, theirs)):
        at = pl.ds(pl.multiple_of((idx_ref[0] ^ flip) * size, size), size)
        for d in range(1, tp):
            acc[:, at] += dot(dqs[d][...], halves[d - 1][...], 1, 1)
    o_ref[...] = norm_back(x_ref[...], g_ref[...], acc[...]).astype(BF16)


def dsource_kernel(idx_ref, x_ref, g_ref, wk_ref, wv_ref, *refs):
    o_ref = refs[KVH]
    total = None
    for r in range(KVH):
        at = pl.ds(pl.multiple_of((idx_ref[0] ^ r) * HD, HD), HD)
        part = dot(refs[r][:, :HD], wk_ref[:, at], 1, 1) + dot(refs[r][:, HD:], wv_ref[:, at], 1, 1)
        total = part if total is None else total + part
    o_ref[...] = norm_back(x_ref[...], g_ref[...], total)


def whole(shape):
    return pl.BlockSpec(shape, lambda *_: (0,) * len(shape))


def estimate(flops, mib):
    return pl.CostEstimate(flops=flops, bytes_accessed=mib << 20, transcendentals=0)


def call(body, out_shape, args, flops=1 << 24, mib=2, mb=12, index=(), scratch=(), specs=None):
    outs = out_shape if isinstance(out_shape, list) else [out_shape]
    specs = specs or [whole(a.shape) for a in args]
    out_specs = [whole(o.shape) for o in outs]
    scalars = [i.astype(jnp.int32).reshape(1) for i in index]
    got = pl.pallas_call(
        body,
        grid_spec=pltpu.PrefetchScalarGridSpec(
            num_scalar_prefetch=len(scalars),
            grid=(1,),
            in_specs=specs,
            out_specs=out_specs,
            scratch_shapes=list(scratch),
        ),
        out_shape=outs,
        compiler_params=pltpu.CompilerParams(vmem_limit_bytes=mb << 20),
        cost_estimate=estimate(flops, mib),
    )(*scalars, *args)
    return got if isinstance(out_shape, list) else got[0]


def in_hbm(*arrays):
    return tuple(pltpu.with_memory_space_constraint(x, pltpu.HBM) for x in arrays)


def local(target, source, target_gain, source_gain, w_query, w_key, w_value, attended, d_attended):
    sp, tp = lax.axis_size("sp"), lax.axis_size("tp")
    me, mt = lax.axis_index("sp"), lax.axis_index("tp")
    rows, dim = target.shape
    srows = source.shape[0]
    width = w_query.shape[1]
    heads = width // HD
    group = tp // KVH
    nb = 4
    nz = sp // nb
    half = nb // 2
    scaling = HD ** (-0.5)
    kv_index = mt // group
    dblk = dim // sp
    steps = 2
    kvw = KVH * HD
    shape = jax.ShapeDtypeStruct
    t_gain, s_gain = target_gain.reshape(1, dim), source_gain.reshape(1, dim)

    hbm = pl.BlockSpec(memory_space=pltpu.HBM)
    near_rows = dim // 2
    by_head = call(
        functools.partial(source_kernel, steps),
        [shape((srows, 2 * HD), BF16)] * KVH,
        in_hbm(source, s_gain, w_key, w_value),
        flops=4 * srows * dim * kvw,
        mb=FRONT_MIB,
        index=(kv_index,),
        specs=[hbm] * 4,
        scratch=[
            pltpu.VMEM((srows, dim), BF16),
            pltpu.VMEM((1, dim), F32),
            pltpu.VMEM((dim, kvw), BF16),
            pltpu.VMEM((dim, kvw), BF16),
            pltpu.VMEM((srows, kvw), BF16),
            pltpu.VMEM((srows, kvw), BF16),
            pltpu.SemaphoreType.DMA((2,)),
            pltpu.SemaphoreType.DMA((steps,)),
            pltpu.SemaphoreType.DMA((steps,)),
        ],
    )
    q_ext, near, far = call(
        functools.partial(target_kernel, steps, sp, half),
        [shape((rows + 16, width), BF16)] + [shape((near_rows, rows), BF16)] * 2,
        in_hbm(target, t_gain, w_query, attended, d_attended),
        flops=2 * rows * dim * width,
        mb=FRONT_MIB,
        index=(me,),
        specs=[hbm] * 5,
        scratch=[
            pltpu.VMEM((rows, dim), BF16),
            pltpu.VMEM((1, dim), F32),
            pltpu.VMEM((dim, width), BF16),
            pltpu.VMEM((rows, width), BF16),
            pltpu.VMEM((rows, width), BF16),
            pltpu.VMEM((dim, rows), BF16),
            pltpu.SemaphoreType.DMA((4,)),
            pltpu.SemaphoreType.DMA((steps,)),
        ],
    )

    def away(x, k, step=None):
        return swap(x, "sp", (step or k) * nb)

    def gathered(blocks):
        odd = [away(blocks[k], k, 1) for k in range(1, nz, 2)]
        pairs = call(
            pair_kernel, [shape(x.shape, BF16) for x in odd[1:]], (*blocks[2::2], *odd[1:]), mib=1
        )
        return [blocks[0], odd[0]] + [away(x, 2 * i + 2) for i, x in enumerate(pairs)]

    rest = [swap(by_head[d // group], "tp", d) for d in range(1, tp)]
    tables = call(cat_kernel, [shape((tp * srows, HD), BF16)] * 2, (by_head[0], *rest), mib=1)
    late = list(range(nz // 2 + 1, nz, 2))
    chunks = [[k for k in range(nz) if k not in late], late]
    chunk_of = {k: c for c, ks in enumerate(chunks) for k in ks}
    key_parts, value_parts = [], []
    for own, places in ((tables[0], key_parts), (tables[1], value_parts)):
        at_hand = {0: own}
        for k in list(range(2, nz, 2)) + list(range(1, nz, 2)):
            at_hand[k] = away(at_hand[k - 1], k, 1) if k % 2 else away(own, k)
        places.extend([[at_hand[k] for k in ks] for ks in chunks])

    def around(x):
        far, near = swap(x, "sp", half), swap(x, "sp", 1)
        return [x, near, far, swap(far, "sp", 1)]

    qs, gs = around(q_ext), around(d_attended)
    far = swap(far, "sp", half)

    held, _ = lax.optimization_barrier((w_query, tables[0]))
    piece = lax.dynamic_slice_in_dim(held, (me & 1) * (dim // 2), dim // 2, 0)
    wq_mine = [swap(piece, "tp", d) for d in range(1, tp)]
    wq_theirs = [swap(w, "sp", 1) for w in wq_mine]

    trows = nb * rows
    stshape = shape((heads, 8, trows), F32)
    dqshape = shape((heads, HD, trows), F32)

    def scores(c):
        parts = key_parts[c]
        part = sum(x.shape[0] for x in parts)
        return call(
            functools.partial(scores_kernel, len(parts), nb, rows, scaling),
            [shape((heads, part, trows), BF16), stshape, shape((HD, part), BF16)],
            (*parts, *qs),
            flops=4 * heads * part * trows * HD,
            scratch=[pltpu.VMEM((part, HD), BF16)],
        )

    def grads(c, probs, keys_t):
        parts = value_parts[c]
        return call(
            functools.partial(grads_kernel, len(parts), nb, rows),
            [shape(probs.shape, BF16), dqshape],
            (*parts, keys_t, probs, *qs, *gs),
            flops=6 * probs.size * HD,
            scratch=[pltpu.VMEM((probs.shape[1], HD), BF16)],
        )

    nc = len(chunks)
    probs, own_stats, keys_t = zip(*[scores(c) for c in range(nc)])
    stats = call(
        functools.partial(lse_kernel, heads),
        shape((8 * -(-heads // 4), trows), F32),
        own_stats,
        mib=1,
    )
    sts = [swap(stats, "sp", k) for k in range(1, nb)]
    d_scores, dq_parts = zip(*[grads(c, probs[c], keys_t[c]) for c in range(nc)])
    coef, sent, kept = call(
        functools.partial(scale_kernel, nc, nb, rows, heads, scaling),
        [stshape, shape((2 * rows, width), BF16), shape((2 * rows, width), F32)],
        (*own_stats, *sts, *dq_parts),
    )
    src = tp * srows
    dkvs = [None] * nz
    for ks in (range(1, nz, 2), range(0, nz, 2)):
        places = [(chunk_of[k], chunks[chunk_of[k]].index(k)) for k in ks]
        results = call(
            functools.partial(keyvalue_kernel, places, nc, nb, rows, scaling),
            [shape((src, 2 * HD), BF16 if k % 2 else F32) for k in ks],
            (*qs, *gs, coef, *probs, *d_scores),
            flops=3 * heads * nz * src * trows * HD,
        )
        for k, x in zip(ks, results):
            dkvs[k] = x

    pair_b = (kept + swap(sent, "sp", 1).astype(F32)).astype(BF16)
    other = swap(pair_b, "sp", half)

    dq_two, dq_own, partial = call(
        functools.partial(first_kernel, nz, dblk, rows),
        [shape((2 * rows, width), BF16), shape((rows, width), BF16), shape((nz * dblk, width), BF16)],
        (pair_b, other, near, far),
        flops=4 * rows * nz * dblk * width,
    )
    got = swap(partial, "sp", 1)
    mine = call(
        functools.partial(second_kernel, nz, dblk),
        [shape((dblk, width), BF16 if k % 2 else F32) for k in range(nz)],
        (dq_two, near, far, got),
        flops=4 * rows * nz * dblk * width,
    )
    d_w_query, *arrived = gathered(mine)
    for x in arrived:
        d_w_query = d_w_query + x.astype(F32)

    dqs = [dq_own] + [swap(dq_own, "tp", d) for d in range(1, tp)]
    d_target = call(
        functools.partial(dtarget_kernel, tp),
        shape((rows, dim), BF16),
        (target, t_gain, *dqs, w_query, *wq_mine, *wq_theirs),
        flops=2 * rows * dim * width * tp,
        index=(me & 1,),
        scratch=[pltpu.VMEM((rows, dim), F32)],
    )

    dkvs = gathered(dkvs)
    own, others = call(
        functools.partial(zsum_kernel, len(dkvs)),
        [shape((srows, 2 * HD), BF16), shape((src - srows, 2 * HD), BF16)],
        dkvs,
    )
    relative = [own] + [None] * (KVH - 1)
    for d in range(1, tp):
        block = swap(others[(d - 1) * srows : d * srows], "tp", d)
        r = d // group
        if relative[r] is None:
            relative[r] = block
        else:
            relative[r] = relative[r].astype(F32) + block.astype(F32)
    d_source = call(
        dsource_kernel,
        shape((srows, dim), F32),
        (source, s_gain, w_key, w_value, *[x.astype(BF16) for x in relative]),
        flops=4 * srows * dim * kvw,
        index=(kv_index,),
    )
    return (d_target, d_source, d_w_query)


def solution(mesh):
    return jax.shard_map(
        local,
        mesh=mesh,
        in_specs=(
            P("sp", None),
            P(("sp", "tp"), None),
            P(),
            P(),
            P(None, "tp"),
            P(),
            P(),
            P("sp", "tp"),
            P("sp", "tp"),
        ),
        out_specs=(P("sp", None), P(("sp", "tp"), None), P("sp", "tp")),
        check_vma=False,
    )
```
